1024 devices in a mesh: rep: 4 (over z_hi), fs: 32 (over z_lo, y), tp: 8 (over x, core).
Axes of the slice: x: 4, y: 4, z: 32 (z_hi: 4, z_lo: 8; z = z_hi * 8 + z_lo), core: 2. Of those that a mesh axis runs over, the one named last changes fastest.
Arguments:
- skip_stream_entry: bfloat16 [32768, 2048], P(('rep', 'fs')), may hold values from -6 to 6
- sequence_blender_factor: float32 [2048], replicated, may hold values from 0.1 to 1.9
- product_projector: float32 [2048, 1024], P('fs', 'tp'), may hold values from -0.125 to 0.125
- product_side_factors: float32 [1024], P('tp'), may hold values from 0.3 to 3
- placewise_projector: float32 [2048, 1024], P('fs', 'tp'), may hold values from -0.125 to 0.125
- placewise_entry_factors: float32 [1024], P('tp'), may hold values from 0.7 to 11.2, as said below
- placewise_rescale_factor: float32 [1024], P('tp'), may hold values from 0.1 to 1.9
- place_cluster_operator: bfloat16 [8, 128, 128], replicated, may hold values from -0.5 to 0.5
- placewise_offset_vector: float32 [8, 128], replicated, may hold values from 0.1 to 1.9
- blender_result_projector: float32 [1024, 2048], P('tp', 'fs'), may hold values from -0.1875 to 0.1875
- blender_result_factors: float32 [2048], P('fs'), may hold values from 0.3 to 3
- feedforward_norm_factor: float32 [2048], replicated, may hold values from 0.1 to 1.9
- switch_projector: float32 [2048, 2816], P('fs', 'tp'), may hold values from -0.125 to 0.125
- switch_factors: float32 [2816], P('tp'), may hold values from 0.3 to 3
- expand_projector: float32 [2048, 2816], P('fs', 'tp'), may hold values from -0.125 to 0.125
- expand_factors: float32 [2816], P('tp'), may hold values from 0.3 to 3
- contract_projector: float32 [2816, 2048], P('tp', 'fs'), may hold values from -0.109375 to 0.109375
- contract_factors: float32 [2048], P('fs'), may hold values from 0.3 to 3
Outputs:
- result: bfloat16 [32768, 2048], P(('rep', 'fs'), 'tp')
The draws below stay inside these ranges and needn't reach their ends.
Inputs may be any that keep to these rules, and one draw needn't show every extreme that they name: `placewise_entry_factors`: positive column scales.
All inputs are finite; a program needn't handle non-finite values.
Results may differ from the reference program's by a relative error of at most 0.023.
Values may be sent and summed in bfloat16 or wider, within the bound.
A program may use at most 32 MiB of HBM per device.

```python
import math
import jax
import jax.numpy as jnp
from jax import lax

EMBED_DIMENSION = 2048
BLENDER_FEATURES = 1024
GROUP_DIM = 128
BLOCK = 128
FF = 2816
SHARED_SEQ_STEPS = 256
GROUPS = 8
TOKENS = 32768
N_REP = 4
N_FS = 32
N_TP = 8


def draw_placewise_entry_factors(key, part):
    column_pos = jnp.arange(BLENDER_FEATURES, dtype=jnp.float32) / (BLENDER_FEATURES - 1)
    rising = jnp.exp(jnp.log(4.0) * column_pos)
    rough_part = jnp.exp(jax.random.uniform(key, (BLENDER_FEATURES,), jnp.float32, jnp.log(0.7), jnp.log(1.4)))
    return rising * rough_part


def levels(stream_key, extent, cuts, least, largest):
    level, own = 1.0, jax.random.fold_in(stream_key, 6)
    for position, shards_of in cuts:
        heights = jnp.exp(jax.random.uniform(jax.random.fold_in(own, position), (shards_of,), jnp.float32, least / len(cuts), largest / len(cuts)))
        level = level * jnp.repeat(heights, extent[position] // shards_of).reshape([-1 if axis == position else 1 for axis in range(len(extent))])
    return level


def bell_draw(rng, dims, scale, reach, split=(), kind=jnp.bfloat16):
    drawn = jax.random.normal(rng, dims, jnp.float32) * scale
    if len(split) > 0:
        drawn = levels(rng, dims, split, -0.22, 0.18) * drawn
    return jnp.clip(drawn, min=-reach, max=reach).astype(kind)


def setup_inputs(seed: int = 0) -> dict:
    key_of = jax.random.split(jax.random.key(seed), 19)
    skip_stream_entry = bell_draw(key_of[0], (TOKENS, EMBED_DIMENSION), 1.0, 6.0, ((0, 128),))
    sequence_blender_factor = jnp.clip(1.0 + 0.18 * jax.random.normal(key_of[1], (EMBED_DIMENSION,), jnp.float32), 0.1, 1.9)
    product_projector = bell_draw(key_of[2], (EMBED_DIMENSION, BLENDER_FEATURES), EMBED_DIMENSION ** -0.5, 0.125, ((0, 32), (1, 8)), jnp.float32)
    product_side_factors = jnp.clip(jnp.exp(math.log(3.0) - 2.3025851 * jax.random.uniform(key_of[3], (BLENDER_FEATURES,), jnp.float32) ** levels(key_of[3], (BLENDER_FEATURES,), ((0, 8),), -0.2, 0.2)), 0.3, 3.0)
    placewise_projector = bell_draw(key_of[4], (EMBED_DIMENSION, BLENDER_FEATURES), EMBED_DIMENSION ** -0.5, 0.125, ((0, 32), (1, 8)), jnp.float32)
    placewise_entry_factors = draw_placewise_entry_factors(jax.random.fold_in(key_of[18], 71), 0)
    placewise_rescale_factor = jnp.clip(1.0 + 0.18 * jax.random.normal(key_of[6], (BLENDER_FEATURES,), jnp.float32), 0.1, 1.9)
    place_cluster_operator = bell_draw(key_of[7], (GROUPS, BLOCK, BLOCK), BLOCK ** -0.5, 0.5)
    placewise_offset_vector = jnp.clip(1.0 + 0.18 * jax.random.normal(key_of[8], (GROUPS, BLOCK), jnp.float32), 0.1, 1.9)
    blender_result_projector = bell_draw(key_of[9], (BLENDER_FEATURES, EMBED_DIMENSION), BLENDER_FEATURES ** -0.5, 0.1875, ((0, 8), (1, 32)), jnp.float32)
    blender_result_factors = jnp.clip(jnp.exp(math.log(3.0) - 2.3025851 * jax.random.uniform(key_of[10], (EMBED_DIMENSION,), jnp.float32) ** levels(key_of[10], (EMBED_DIMENSION,), ((0, 32),), -0.2, 0.2)), 0.3, 3.0)
    feedforward_norm_factor = jnp.clip(1.0 + 0.18 * jax.random.normal(key_of[11], (EMBED_DIMENSION,), jnp.float32), 0.1, 1.9)
    switch_projector = bell_draw(key_of[12], (EMBED_DIMENSION, FF), EMBED_DIMENSION ** -0.5, 0.125, ((0, 32), (1, 8)), jnp.float32)
    switch_factors = jnp.clip(jnp.exp(math.log(3.0) - 2.3025851 * jax.random.uniform(key_of[13], (FF,), jnp.float32) ** levels(key_of[13], (FF,), ((0, 8),), -0.2, 0.2)), 0.3, 3.0)
    expand_projector = bell_draw(key_of[14], (EMBED_DIMENSION, FF), EMBED_DIMENSION ** -0.5, 0.125, ((0, 32), (1, 8)), jnp.float32)
    expand_factors = jnp.clip(jnp.exp(math.log(3.0) - 2.3025851 * jax.random.uniform(key_of[15], (FF,), jnp.float32) ** levels(key_of[15], (FF,), ((0, 8),), -0.2, 0.2)), 0.3, 3.0)
    contract_projector = bell_draw(key_of[16], (FF, EMBED_DIMENSION), FF ** -0.5, 0.109375, ((0, 8), (1, 32)), jnp.float32)
    contract_factors = jnp.clip(jnp.exp(math.log(3.0) - 2.3025851 * jax.random.uniform(key_of[17], (EMBED_DIMENSION,), jnp.float32) ** levels(key_of[17], (EMBED_DIMENSION,), ((0, 32),), -0.2, 0.2)), 0.3, 3.0)
    return dict(skip_stream_entry=skip_stream_entry, sequence_blender_factor=sequence_blender_factor, product_projector=product_projector, product_side_factors=product_side_factors, placewise_projector=placewise_projector, placewise_entry_factors=placewise_entry_factors, placewise_rescale_factor=placewise_rescale_factor, place_cluster_operator=place_cluster_operator, placewise_offset_vector=placewise_offset_vector, blender_result_projector=blender_result_projector, blender_result_factors=blender_result_factors, feedforward_norm_factor=feedforward_norm_factor, switch_projector=switch_projector, switch_factors=switch_factors, expand_projector=expand_projector, expand_factors=expand_factors, contract_projector=contract_projector, contract_factors=contract_factors)


epsilon = 1e-06

def normalize(values, gain):
    return values * lax.rsqrt(lax.optimization_barrier(jnp.mean(values * values, axis=-1, keepdims=True)) + epsilon) * gain

def shard_total(activations, weight, scale):
    shards = activations.astype(jnp.float32).reshape(activations.shape[0], N_TP, -1)
    pieces = weight.astype(jnp.float32).reshape(N_TP, -1, weight.shape[1])
    partial_value = jnp.einsum('tkc,kcd->ktd', shards, pieces) * scale
    rounded = lax.optimization_barrier(partial_value.astype(jnp.bfloat16))
    return lax.optimization_barrier(jnp.sum(rounded.astype(jnp.float32), axis=0))

def reference(skip_stream_entry, sequence_blender_factor, product_projector, product_side_factors, placewise_projector, placewise_entry_factors, placewise_rescale_factor, place_cluster_operator, placewise_offset_vector, blender_result_projector, blender_result_factors, feedforward_norm_factor, switch_projector, switch_factors, expand_projector, expand_factors, contract_projector, contract_factors):
    product_lowered = product_projector.astype(jnp.bfloat16)
    spread_low = placewise_projector.astype(jnp.bfloat16)
    mix_out_low = blender_result_projector.astype(jnp.bfloat16)
    gate_low = switch_projector.astype(jnp.bfloat16)
    up_low = expand_projector.astype(jnp.bfloat16)
    down_low = contract_projector.astype(jnp.bfloat16)
    causal = jnp.tril(jnp.ones((BLOCK, BLOCK), dtype=bool))
    masked = jnp.where(causal[None], place_cluster_operator, jnp.zeros_like(place_cluster_operator)).astype(jnp.float32)

    def layer(rows):
        standardized_stream = normalize(rows.astype(jnp.float32), sequence_blender_factor).astype(jnp.bfloat16)
        product_portion = jax.nn.gelu(jnp.dot(standardized_stream, product_lowered, preferred_element_type=jnp.float32) * product_side_factors)
        spread = jax.nn.gelu(jnp.dot(standardized_stream, spread_low, preferred_element_type=jnp.float32) * placewise_entry_factors)
        spread_normed = normalize(spread, placewise_rescale_factor).astype(jnp.bfloat16)
        blocks = spread_normed.astype(jnp.float32).reshape(SHARED_SEQ_STEPS // BLOCK, BLOCK, GROUPS, GROUP_DIM)
        blended_sequence = jnp.einsum('gts,nsgc->ntgc', masked, blocks, precision=lax.Precision.HIGHEST)
        blended_sequence = blended_sequence + placewise_offset_vector.T[None, :, :, None]
        switched_inner = (product_portion * blended_sequence.reshape(SHARED_SEQ_STEPS, BLENDER_FEATURES)).astype(jnp.bfloat16)
        stream = (rows.astype(jnp.float32) + shard_total(switched_inner, mix_out_low, blender_result_factors)).astype(jnp.bfloat16)
        ffn_normed = normalize(stream.astype(jnp.float32), feedforward_norm_factor).astype(jnp.bfloat16)
        gate = jnp.dot(ffn_normed, gate_low, preferred_element_type=jnp.float32) * switch_factors
        upper = jnp.dot(ffn_normed, up_low, preferred_element_type=jnp.float32) * expand_factors
        active = (jax.nn.silu(gate) * upper).astype(jnp.bfloat16)
        return (stream.astype(jnp.float32) + shard_total(active, down_low, contract_factors)).astype(jnp.bfloat16)
    grouped = skip_stream_entry.reshape(N_REP * N_FS, SHARED_SEQ_STEPS, EMBED_DIMENSION)
    return lax.map(layer, grouped).reshape(TOKENS, EMBED_DIMENSION)
```

```python
import functools

import jax
import jax.numpy as jnp
from jax import lax
from jax.experimental import pallas as pl
from jax.experimental.pallas import tpu as pltpu
from jax.sharding import PartitionSpec as P

EPS = 1e-06
F32 = jnp.float32
BF16 = jnp.bfloat16
MESH = pl.DeviceIdType.MESH

TOK = 256
BLOCK = 128
DIM = 2048
CH = 1024
HID = 352
NY, NZ, NX, NTP, NREP = 4, 8, 4, 8, 4

R_PROD, R_PLACE, R_BLEND, R_SE, R_CON, R_ALL = 0, 64, 128, 192, 576, 768

RING4 = {1: 0, 2: 1, 3: 2, 4: 3, -1: 0, -2: -1, -3: -2}
RING3 = {1: 0, 2: 1, 3: 2, -1: 0, -2: -1, -3: -2, -4: -3}
JUMP4 = {1: 0, 2: 0, 3: 2, 4: 2, -1: 0, -2: 0, -3: -2}
JUMP3 = {1: 0, 2: 0, 3: 2, -1: 0, -2: 0, -3: -2, -4: -2}
FAR4 = {1: 0, 2: 0, 3: 0, 4: 0, -1: 0, -2: 0, -3: 0}
FAR3 = {1: 0, 2: 0, 3: 0, -1: 0, -2: 0, -3: 0, -4: 0}
YUP = {1: 0, -1: 0, 2: 1}
YDN = {1: 0, -1: 0, -2: -1}
YUP2 = {1: 0, -1: 0, 2: 0}
YDN2 = {1: 0, -1: 0, -2: 0}

STREAMS = (
    (R_PROD, 64, "z", JUMP4, YUP, 0.0),
    (R_PLACE, 64, "y", JUMP3, YDN, 0.0),
    (R_BLEND, 64, "y", RING4, YDN, 0.0),
    (R_SE, 128, "z", RING3, YUP, 4.0),
    (R_SE + 128, 128, "z", RING4, YDN, 8.0),
    (R_SE + 256, 128, "z", RING3, YUP, 10.0),
    (R_CON, 192, "y", RING4, YDN, 12.0),
)
IN, BLEND, SE, CON = (0, 1), (2,), (3, 4, 5), (6,)


def order_of(tree):
    return sorted(tree, key=lambda d: (abs(d), -d))


def arrivals_of(stream):
    first, zt, yt = stream[2:5]
    out = {}
    if first == "z":
        for dz in order_of(zt):
            out[(dz, 0)] = ((zt[dz], 0), "z", dz - zt[dz])
        for dz in [0, *order_of(zt)]:
            for dy in order_of(yt):
                out[(dz, dy)] = ((dz, yt[dy]), "y", dy - yt[dy])
    else:
        for dy in order_of(yt):
            out[(0, dy)] = ((0, yt[dy]), "y", dy - yt[dy])
        for dy in [0, *order_of(yt)]:
            for dz in order_of(zt):
                out[(dz, dy)] = ((zt[dz], dy), "z", dz - zt[dz])
    return out


class Plan:
    def __init__(self):
        self.tasks = {}
        self.copies = {}

    def copy(self, key, link, size, hops):
        self.copies[key] = len(self.copies)
        return (key, link, size, hops)

    def task(self, key, deps, dur, sends=(), rank=1, begin=0.0):
        self.tasks[key] = (tuple(deps), dur, tuple(sends), rank, begin)

    def order(self):
        t, arrived, free, done, seq = 0.0, {}, {}, {}, []
        left = dict(self.tasks)
        while left:
            best, when = None, None
            for key, (deps, _, _, rank, begin) in left.items():
                ready = begin
                for d in deps:
                    at = done.get(d) if d in self.tasks else arrived.get(d)
                    if at is None:
                        ready = None
                        break
                    ready = max(ready, at)
                if ready is None:
                    continue
                mark = (max(ready, t), rank, ready)
                if when is None or mark < when:
                    best, when = key, mark
            deps, dur, sends, *_ = left.pop(best)
            t = max(t, when[0]) + dur
            done[best] = t
            for key, link, size, hops in sends:
                rate = 650e3 if link == "d2d" else 46.6e3
                begin = max(free.get(link, 0.0), t)
                wire = size * max(hops, 1) / rate
                free[link] = begin + wire
                arrived[key] = begin + wire + (1.0 if link == "d2d" else 1.4 + 0.75 * hops)
            seq.append((best, t))
        return seq


def make_plan():
    plan = Plan()
    stream_tasks = {}
    plan.task("pack1", [], 2.0)
    plan.task("pack2", ["pack1"], 0.5, (), 2)
    plan.task("pack3", ["pack1"], 0.5, (), 3)
    for s, stream in enumerate(STREAMS):
        arr = arrivals_of(stream)
        sends = {}
        for a, (parent, axis, step) in arr.items():
            key = ("w", s, *a)
            link = axis + ("+" if step > 0 else "-")
            cp = plan.copy(key, link, stream[1] * 256, abs(step))
            sends.setdefault(parent, []).append(cp)
        pack = "pack1" if s in IN + BLEND else "pack2" if s in SE else "pack3"
        plan.task(("go", s), [pack], 0.03, sends[(0, 0)], 0, stream[5])
        for a in arr:
            key = ("w", s, *a)
            plan.task(("recv", s, *a), [key, ("go", s)], 0.03, sends.get(a, ()), 0)
        stream_tasks[s] = [("recv", s, *a) for a in arr]
    def whole(which):
        return [t for s in which for t in stream_tasks[s]]

    plan.task("norm", ["pack1"], 1.5, (), 2)
    sq = [plan.copy(("sq", k), "d2d" if k == 4 else "q", 1024, 1) for k in range(1, NTP)]
    plan.task("in", ["norm", *whole(IN)], 1.5, sq, 2)
    plan.task("mask", ["pack1"], 0.2, (), 3)
    plan.task("mixed", ["in", "mask", *[("sq", k) for k in range(1, NTP)]], 0.8, (), 1)

    def scatter(w, deps, dur):
        last = deps
        for k in (2, 1, 3, 0):
            cp = plan.copy(("p", w, k), "d2d", 131072, 1)
            plan.task(("part", w, k), last, dur, (cp,), 1)
            last = [("part", w, k)]
        for k in (2, 1, 3, 0):
            cps = ()
            if k:
                cps = (plan.copy(("c", w, k), "x-" if k == 3 else "x+", 131072, 2 if k == 2 else 1),)
            plan.task(("sum", w, k), [*last, ("p", w, k)], dur + 0.1, cps, 1)
            last = [("sum", w, k)]
        return [*last, *[("c", w, k) for k in (1, 2, 3)]]

    after = scatter(0, ["mixed", *whole(BLEND)], 0.2)
    ag = [plan.copy(("ap", 0), "d2d", 131072, 1)]
    for k in (2, 1, 3):
        ag.append(plan.copy(("ac", k), "x-" if k == 3 else "x+", 131072, 2 if k == 2 else 1))
    plan.task("stream", after, 0.3, ag, 1)
    for k in (1, 3, 2):
        plan.task(("pass", k), [("ac", k), "stream"], 0.03, (plan.copy(("ap", k), "d2d", 131072, 1),), 0)
    got = [("pass", k) for k in (1, 2, 3)] + [("ap", k) for k in range(4)]
    plan.task("norm2", ["stream", *got], 1.5, (), 1)
    plan.task("hidden", ["norm2", *whole(SE)], 3.0, (), 1)
    after = scatter(1, ["hidden", *whole(CON)], 0.3)
    plan.task("out", after, 0.3, (), 1)
    return plan


def kernel(
    plan,
    seq,
    x_ref,
    gain1_ref,
    wprod_ref,
    sprod_ref,
    wplace_ref,
    splace_ref,
    gains_ref,
    op_ref,
    bias_ref,
    wblend_ref,
    sblend_ref,
    gain2_ref,
    wsw_ref,
    ssw_ref,
    wex_ref,
    sex_ref,
    wcon_ref,
    scon_ref,
    out_ref,
    g,
    normed,
    carrier,
    spread,
    sqbuf,
    opm,
    gated,
    active,
    psend,
    precv,
    csend,
    crecv,
    own,
    sbuf,
    scale,
    send_sem,
    recv_sem,
):
    rep, fs, tp = lax.axis_index("rep"), lax.axis_index("fs"), lax.axis_index("tp")
    zl, y = fs // NY, lax.rem(fs, NY)
    x, core = tp // 2, lax.rem(tp, 2)
    z = rep * NZ + zl

    def at_z(d):
        zz = lax.rem(z + d + NREP * NZ, NREP * NZ)
        return {"rep": zz // NZ, "fs": lax.rem(zz, NZ) * NY + y}

    def at_y(d):
        return {"fs": zl * NY + lax.rem(y + d + NY, NY)}

    def at_tp(k):
        return {"tp": lax.rem(tp + k + NTP, NTP)}

    def at_x(k):
        return {"tp": lax.rem(x + k + NX, NX) * 2 + core}

    partner = {"tp": x * 2 + 1 - core}

    def slot(a):
        return lax.rem(zl - a[0] + NZ, NZ) * NY + lax.rem(y - a[1] + NY, NY)

    pending = []

    def send(key, src, dst, dev):
        i = plan.copies[key]
        cp = pltpu.make_async_remote_copy(
            src_ref=src, dst_ref=dst, send_sem=send_sem.at[i], recv_sem=recv_sem.at[i],
            device_id=dev, device_id_type=MESH,
        )
        cp.start()
        pending.append(cp)

    def arrive(key, dst, dev):
        i = plan.copies[key]
        pltpu.make_async_remote_copy(
            src_ref=dst, dst_ref=dst, send_sem=send_sem.at[i], recv_sem=recv_sem.at[i],
            device_id=dev, device_id_type=MESH,
        ).wait_recv()

    arrs = [arrivals_of(s) for s in STREAMS]

    def block(s, a):
        return g.at[slot(a), pl.ds(STREAMS[s][0], STREAMS[s][1])]

    def forward(s, a):
        for b, (parent, axis, step) in arrs[s].items():
            if parent == a:
                send(("w", s, *b), block(s, a), block(s, a), at_z(step) if axis == "z" else at_y(step))

    zs = sorted({e * v[2] for a in arrs for v in a.values() if v[1] == "z" for e in (1, -1)})
    ys = sorted({(e * v[2]) % NY for a in arrs for v in a.values() if v[1] == "y" for e in (1, -1)})
    greet = [at_z(d) for d in zs] + [at_y(d) for d in ys] + [at_tp(k) for k in range(1, NTP)]
    barrier = pltpu.get_barrier_semaphore()
    for dev in greet:
        pl.semaphore_signal(barrier, inc=1, device_id=dev, device_id_type=MESH)

    def pack1():
        g[fs, R_PROD : R_PROD + 64, :] = wprod_ref[...].astype(BF16)
        g[fs, R_PLACE : R_PLACE + 64, :] = wplace_ref[...].astype(BF16)
        wb = (wblend_ref[...].astype(BF16).astype(F32) * sblend_ref[...]).T
        g[fs, R_BLEND : R_BLEND + 64, :] = wb.astype(BF16)
        pl.semaphore_wait(barrier, len(greet))

    def pack2():
        for i, w in ((0, wsw_ref), (2, wex_ref)):
            for j in (0, 1):
                g[fs, R_SE + 64 * (i + j) : R_SE + 64 * (i + j + 1), :] = w[:, 128 * j : 128 * (j + 1)].astype(BF16)
        zero = jnp.zeros((64, 128), BF16)
        for i, w in ((4, wsw_ref), (5, wex_ref)):
            g[fs, R_SE + 64 * i : R_SE + 64 * (i + 1), :] = zero
            g[fs, R_SE + 64 * i : R_SE + 64 * (i + 1), 0:96] = w[:, 256:352].astype(BF16)
        scale[...] = jnp.zeros_like(scale)
        scale[0:1, 0:HID] = ssw_ref[...]
        scale[1:2, 0:HID] = sex_ref[...]

    def pack3():
        wc = (wcon_ref[...].astype(BF16).astype(F32) * scon_ref[...]).T.astype(BF16)
        g[fs, R_CON : R_CON + 64, :] = wc[:, 0:128]
        g[fs, R_CON + 64 : R_CON + 128, :] = wc[:, 128:256]
        g[fs, R_CON + 128 : R_CON + 192, :] = jnp.zeros((64, 128), BF16)
        g[fs, R_CON + 128 : R_CON + 192, 0:96] = wc[:, 256:352]

    def go(s):
        forward(s, (0, 0))

    def recv(s, dz, dy):
        _, axis, step = arrs[s][(dz, dy)]
        arrive(("w", s, dz, dy), block(s, (dz, dy)), at_z(-step) if axis == "z" else at_y(-step))
        forward(s, (dz, dy))

    def tile(row):
        return g[:, row : row + 64, :].reshape(DIM, 128)

    def norm():
        v = x_ref[...].astype(F32)
        r = lax.rsqrt(jnp.mean(v * v, axis=-1, keepdims=True) + EPS)
        normed[...] = (v * r * gain1_ref[...]).astype(BF16)

    def enter():
        w = jnp.concatenate([tile(R_PROD), tile(R_PLACE)], axis=1)
        h = jnp.dot(normed[...], w, preferred_element_type=F32)
        sp = jax.nn.gelu(h[:, 128:256] * splace_ref[...])
        spread[...] = sp
        sqbuf[tp] = jnp.sum((sp * sp).T, axis=0, keepdims=True)
        for k in range(1, NTP):
            send(("sq", k), sqbuf.at[tp], sqbuf.at[tp], at_tp(k))
        carrier[...] = jax.nn.gelu(h[:, 0:128] * sprod_ref[...])

    def mask():
        t = lax.broadcasted_iota(jnp.int32, (BLOCK, BLOCK), 0)
        s = lax.broadcasted_iota(jnp.int32, (BLOCK, BLOCK), 1)
        opm[...] = jnp.where(t >= s, op_ref[tp].astype(F32), 0.0).astype(BF16)

    def mixed():
        for k in range(1, NTP):
            src = lax.rem(tp - k + NTP, NTP)
            arrive(("sq", k), sqbuf.at[src], at_tp(-k))
        total = jnp.sum(sqbuf[...], axis=0)
        r = lax.rsqrt(total / CH + EPS)
        r = jnp.broadcast_to(r, (128, TOK)).T
        sn = (spread[...] * r * gains_ref[...]).astype(BF16)
        bias = jnp.broadcast_to(bias_ref[pl.ds(tp, 1), :], (BLOCK, BLOCK)).T
        w = opm[...]
        for n in range(TOK // BLOCK):
            rows = slice(n * BLOCK, (n + 1) * BLOCK)
            m = jnp.dot(w, sn[rows], preferred_element_type=F32) + bias
            gated[rows, :] = (carrier[rows, :] * m).astype(BF16)

    nt = (((1,), (1,)), ((), ()))

    def product(w, d):
        if w == 0:
            b = g[pl.ds(4 * d, 4), R_BLEND : R_BLEND + 64, :].reshape(256, 128)
            return lax.dot_general(gated[...], b, nt, preferred_element_type=F32)
        cols = [g[pl.ds(4 * d, 4), R_CON + 64 * j : R_CON + 64 * (j + 1), :].reshape(256, 128) for j in range(3)]
        return lax.dot_general(active[...], jnp.concatenate(cols, axis=1), nt, preferred_element_type=F32)

    def chip(k):
        return lax.rem(x + k, NX) * 2

    def part(w, k):
        psend[w, k] = product(w, chip(k) + 1 - core).astype(BF16)
        send(("p", w, k), psend.at[w, k], precv.at[w, k], partner)

    def add(w, k):
        v = product(w, chip(k) + core)
        arrive(("p", w, k), precv.at[w, k], partner)
        v = v + precv[w, k].astype(F32)
        if k == 0:
            own[...] = v
        else:
            csend[w, k - 1] = v.astype(BF16)
            send(("c", w, k), csend.at[w, k - 1], crecv.at[w, k - 1], at_x(k))

    def total(w):
        v = own[...]
        for k in (1, 2, 3):
            arrive(("c", w, k), crecv.at[w, k - 1], at_x(-k))
            v = v + crecv[w, k - 1].astype(F32)
        return v

    def stream():
        mine = x_ref[:, pl.ds(pl.multiple_of(tp * 256, 256), 256)].astype(F32)
        sbuf[tp] = (mine + total(0)).astype(BF16)
        for k in (2, 1, 3):
            send(("ac", k), sbuf.at[tp], sbuf.at[tp], at_x(k))
        send(("ap", 0), sbuf.at[tp], sbuf.at[tp], partner)

    def relay(k):
        d = lax.rem(x - k + NX, NX) * 2 + core
        arrive(("ac", k), sbuf.at[d], at_x(-k))
        send(("ap", k), sbuf.at[d], sbuf.at[d], partner)

    def norm2():
        for k in range(4):
            d = lax.rem(x - k + NX, NX) * 2 + 1 - core
            arrive(("ap", k), sbuf.at[d], partner)
        sq = jnp.zeros((TOK, 256), F32)
        for d in range(NTP):
            v = sbuf[d].astype(F32)
            sq = sq + v * v
        r = lax.rsqrt(jnp.sum(sq, axis=-1, keepdims=True) / DIM + EPS)
        for d in range(NTP):
            cols = slice(256 * d, 256 * (d + 1))
            normed[:, cols] = (sbuf[d].astype(F32) * r * gain2_ref[:, cols]).astype(BF16)

    def hidden():
        for j, (a, b) in enumerate(((0, 2), (1, 3), (4, 5))):
            w = jnp.concatenate([tile(R_SE + 64 * a), tile(R_SE + 64 * b)], axis=1)
            h = jnp.dot(normed[...], w, preferred_element_type=F32)
            cols = slice(128 * j, 128 * (j + 1))
            gate = h[:, 0:128] * scale[0:1, cols]
            up = h[:, 128:256] * scale[1:2, cols]
            active[:, cols] = (gate / (1.0 + jnp.exp(-gate)) * up).astype(BF16)

    def out():
        out_ref[...] = (sbuf[tp].astype(F32) + total(1)).astype(BF16)

    run = {
        "pack1": pack1, "pack2": pack2, "pack3": pack3, "go": go, "norm": norm, "in": enter, "mask": mask, "mixed": mixed, "stream": stream,
        "norm2": norm2, "hidden": hidden, "out": out, "recv": recv, "part": part, "sum": add, "pass": relay,
    }
    for key, _ in seq:
        if isinstance(key, tuple):
            run[key[0]](*key[1:])
        else:
            run[key]()
    for cp in pending:
        cp.wait_send()


def on_device(*args):
    plan = make_plan()
    seq = plan.order()
    n = len(plan.copies)
    args = [a.reshape(1, -1) if a.ndim == 1 else a for a in args]
    return pl.pallas_call(
        functools.partial(kernel, plan, seq),
        out_shape=jax.ShapeDtypeStruct((TOK, 256), BF16),
        in_specs=[pl.BlockSpec(memory_space=pltpu.VMEM)] * len(args),
        out_specs=pl.BlockSpec(memory_space=pltpu.VMEM),
        scratch_shapes=[
            pltpu.VMEM((NY * NZ, R_ALL, 128), BF16),
            pltpu.VMEM((TOK, DIM), BF16),
            pltpu.VMEM((TOK, 128), F32),
            pltpu.VMEM((TOK, 128), F32),
            pltpu.VMEM((NTP, 1, TOK), F32),
            pltpu.VMEM((BLOCK, BLOCK), BF16),
            pltpu.VMEM((TOK, 128), BF16),
            pltpu.VMEM((TOK, 384), BF16),
            pltpu.VMEM((2, 4, TOK, 256), BF16),
            pltpu.VMEM((2, 4, TOK, 256), BF16),
            pltpu.VMEM((2, 3, TOK, 256), BF16),
            pltpu.VMEM((2, 3, TOK, 256), BF16),
            pltpu.VMEM((TOK, 256), F32),
            pltpu.VMEM((NTP, TOK, 256), BF16),
            pltpu.VMEM((8, 384), F32),
            pltpu.SemaphoreType.DMA((n,)),
            pltpu.SemaphoreType.DMA((n,)),
        ],
        compiler_params=pltpu.CompilerParams(
            collective_id=0, has_side_effects=True, vmem_limit_bytes=48 * 1024 * 1024
        ),
        name="layer",
    )(*args)


def solution(mesh):
    return jax.shard_map(
        on_device,
        mesh=mesh,
        in_specs=(
            P(("rep", "fs"), None),
            P(),
            P("fs", "tp"),
            P("tp"),
            P("fs", "tp"),
            P("tp"),
            P("tp"),
            P(),
            P(),
            P("tp", "fs"),
            P("fs"),
            P(),
            P("fs", "tp"),
            P("tp"),
            P("fs", "tp"),
            P("tp"),
            P("tp", "fs"),
            P("fs"),
        ),
        out_specs=P(("rep", "fs"), "tp"),
        check_vma=False,
    )
```

```python
import functools

import jax
import jax.numpy as jnp
from jax import lax
from jax.experimental import pallas as pl
from jax.experimental.pallas import tpu as pltpu
from jax.sharding import PartitionSpec as P

EPS = 1e-06
F32 = jnp.float32
BF16 = jnp.bfloat16
MESH = pl.DeviceIdType.MESH

TOK = 256
BLOCK = 128
DIM = 2048
CH = 1024
HID = 352
NY, NZ, NX, NTP, NREP = 4, 8, 4, 8, 4

R_PROD, R_PLACE, R_BLEND, R_SE, R_CON, R_ALL = 0, 64, 128, 192, 576, 768

RING4 = {1: 0, 2: 1, 3: 2, 4: 3, -1: 0, -2: -1, -3: -2}
RING3 = {1: 0, 2: 1, 3: 2, -1: 0, -2: -1, -3: -2, -4: -3}
JUMP4 = {1: 0, 2: 0, 3: 2, 4: 2, -1: 0, -2: 0, -3: -2}
JUMP3 = {1: 0, 2: 0, 3: 2, -1: 0, -2: 0, -3: -2, -4: -2}
FAR4 = {1: 0, 2: 0, 3: 0, 4: 0, -1: 0, -2: 0, -3: 0}
FAR3 = {1: 0, 2: 0, 3: 0, -1: 0, -2: 0, -3: 0, -4: 0}
YUP = {1: 0, -1: 0, 2: 1}
YDN = {1: 0, -1: 0, -2: -1}
YUP2 = {1: 0, -1: 0, 2: 0}
YDN2 = {1: 0, -1: 0, -2: 0}

KINDS = ("w", "sq", "p", "c", "ac", "ap")
NAMES = (
    "x", "gain1", "wprod", "sprod", "wplace", "splace", "gains", "op", "bias",
    "wblend", "sblend", "gain2", "wsw", "ssw", "wex", "sex", "wcon", "scon",
)
LOADS = (
    "wprod", "wplace", "wblend", "sblend", "wsw", "wex", "wcon", "scon", "x", "gain1", "sprod", "splace",
    "op", "gains", "bias", "ssw", "sex", "gain2",
)

STREAMS = (
    (0, 64, "z", JUMP4, YDN, 0.0, 0.0),
    (64, 64, "z", JUMP3, YUP, 0.0, 0.0),
    (128, 64, "z", JUMP3, YDN, 2.5, 0.0),
    (192, 128, "z", RING4, YUP, 12.2, 1.0),
    (320, 128, "z", JUMP3, YDN, 13.6, 1.0),
    (448, 128, "y", RING3, YUP, 0, 1.0),
    (576, 192, "y", RING4, YUP, 13.2, 1.0),
)
IN, BLEND, SE, CON = (0, 1), (2,), (3, 4, 5), (6,)


def order_of(tree):
    return sorted(tree, key=lambda d: (abs(d), -d))


def arrivals_of(stream):
    first, zt, yt = stream[2:5]
    out = {}
    if first == "z":
        for dz in order_of(zt):
            out[(dz, 0)] = ((zt[dz], 0), "z", dz - zt[dz])
        for dz in [0, *order_of(zt)]:
            for dy in order_of(yt):
                out[(dz, dy)] = ((dz, yt[dy]), "y", dy - yt[dy])
    else:
        for dy in order_of(yt):
            out[(0, dy)] = ((0, yt[dy]), "y", dy - yt[dy])
        for dy in [0, *order_of(yt)]:
            for dz in order_of(zt):
                out[(dz, dy)] = ((zt[dz], dy), "z", dz - zt[dz])
    return out


def leaves_of(arrivals):
    parents = {v[0] for v in arrivals.values()}
    return [a for a in arrivals if a not in parents]


class Plan:
    def __init__(self):
        self.tasks = {}
        self.copies = {}
        self.groups = {}

    def copy(self, key, link, size, hops, group=None):
        self.copies[key] = self.groups.setdefault(group or key, len(self.groups))
        return (key, link, size, hops)

    def task(self, key, deps, dur, sends=(), rank=1, begin=0.0, slack=0.0):
        self.tasks[key] = (tuple(deps), dur, tuple(sends), rank, begin, slack)

    def order(self):
        t, arrived, free, done, seq = 0.0, {}, {}, {}, []
        waits = {k: sum(1 for _ in v[0]) for k, v in self.tasks.items()}
        users, ready, open_ = {}, {k: v[4] for k, v in self.tasks.items()}, set()
        for k, v in self.tasks.items():
            for d in v[0]:
                users.setdefault(d, []).append(k)
            if not waits[k]:
                open_.add(k)

        def came(d, at):
            for k in users.get(d, ()):
                waits[k] -= 1
                ready[k] = max(ready[k], at + (self.tasks[k][5] if d not in self.tasks else 0.0))
                if not waits[k]:
                    open_.add(k)

        index = {k: i for i, k in enumerate(self.tasks)}
        while open_:
            best = min(open_, key=lambda k: (max(ready[k], t), self.tasks[k][3], ready[k], index[k]))
            open_.remove(best)
            _, dur, sends, *_ = self.tasks[best]
            t = max(t, ready[best]) + dur
            came(best, t)
            for key, link, size, hops in sends:
                rate = 650e3 if link == "d2d" else 46.6e3
                begin = max(free.get(link, 0.0), t)
                wire = size * max(hops, 1) / rate
                free[link] = begin + wire
                came(key, begin + wire + (1.0 if link == "d2d" else 0.95 + 0.75 * hops))
            seq.append((best, t))
        assert len(seq) == len(self.tasks)
        return seq


def make_plan():
    plan = Plan()
    stream_tasks = {}
    plan.task("pack1", [], 1.5)
    plan.task("pack2", ["pack1"], 0.1, (), 2)
    plan.task("pack3", ["pack1"], 0.2, (), 2)
    for s, stream in enumerate(STREAMS):
        arr = arrivals_of(stream)
        leaves = leaves_of(arr)
        sends = {}
        for a, (parent, axis, step) in arr.items():
            key = ("w", s, *a)
            link = axis + ("+" if step > 0 else "-")
            cp = plan.copy(key, link, stream[1] * 256, abs(step), ("leaf", s) if a in leaves else key)
            sends.setdefault(parent, []).append(cp)
        pack = "pack1" if s in IN + BLEND else "pack2" if s in SE else "pack3"
        plan.task(("go", s), [pack], 0.03, sends[(0, 0)], 0, stream[5])
        for a in arr:
            if a not in leaves:
                plan.task(("recv", s, *a), [("w", s, *a), ("go", s)], 0.03, sends[a], 0, 0.0, stream[6])
        plan.task(("leaf", s), [("go", s), *[("w", s, *a) for a in leaves]], 0.03, (), 1)
        stream_tasks[s] = [("recv", s, *a) for a in arr if a not in leaves] + [("leaf", s)]

    def whole(which):
        return [t for s in which for t in stream_tasks[s]]

    plan.task("norm", ["pack1"], 0.45, (), 2)
    sq = [plan.copy(("sq", k), "d2d" if k == 4 else "q", 1024, 1) for k in range(1, NTP)]
    plan.task("in", ["norm", *whole(IN)], 0.9, sq, 2)
    plan.task("mask", ["pack1"], 0.03, (), 3)
    plan.task("mixed", ["in", "mask", *[("sq", k) for k in range(1, NTP)]], 0.45, (), 1)

    half = 65536

    def scatter(w, deps, dur):
        last = deps
        for k in (2, 1, 3, 0):
            cp = plan.copy(("p", w, k), "d2d", 2 * half, 1)
            plan.task(("part", w, k), last, dur, (cp,), 1)
            last = [("part", w, k)]
        cps = [plan.copy(("c", w, 2, h), "x-" if h else "x+", half, 1) for h in (0, 1)]
        plan.task(("sum2", w), [*last, ("p", w, 2)], dur + 0.1, cps, 1)
        last = [("sum2", w)]
        for k, h in ((1, 1), (3, 0), (1, 0), (3, 1)):
            cp = plan.copy(("c", w, k, h), "x-" if k == 3 else "x+", half, 1)
            need = [("c", w, 2, h)] if (k, h) in ((1, 0), (3, 1)) else []
            plan.task(("sum", w, k, h), [*last, *need, ("p", w, k)], dur * 0.6 + 0.1, (cp,), 1)
        plan.task(("own", w), [*last, ("p", w, 0)], dur, (), 2)
        return [("own", w)] + [("c", w, k, h) for k in (1, 3) for h in (0, 1)]

    after = scatter(0, ["mixed", *whole(BLEND)], 0.2)
    ag = [plan.copy(("ac", k, h), "x-" if k == 3 else "x+", half, 1) for k, h in ((1, 0), (3, 1), (1, 1), (3, 0))]
    ag.append(plan.copy(("ap", 0, 0), "d2d", 2 * half, 1))
    plan.task("stream", after, 0.2, ag, 1)
    got = [("ap", 0, 0)]
    for k, h in ((1, 0), (3, 1), (1, 1), (3, 0), (2, 0), (2, 1)):
        cps = []
        if (k, h) in ((1, 0), (3, 1)):
            cps.append(plan.copy(("ac", 2, h), "x-" if h else "x+", half, 1))
        cps.append(plan.copy(("ap", k, h), "d2d", half, 1))
        plan.task(("pass", k, h), [("ac", k, h), "stream"], 0.03, cps, 0)
        got += [("pass", k, h), ("ap", k, h)]
    plan.task("norm2", ["stream", *got], 0.5, (), 1)
    plan.task("hidden", ["norm2", *whole(SE)], 1.3, (), 1)
    after = scatter(1, ["hidden", *whole(CON)], 0.3)
    plan.task("out", after, 0.3, (), 1)
    return plan


def kernel(
    plan,
    seq,
    *refs,
):
    hbm, out_ref, rest = refs[: len(NAMES)], refs[len(NAMES)], refs[len(NAMES) + 1 :]
    local, rest = rest[: len(NAMES)], rest[len(NAMES) :]
    (
        g,
        normed,
        carrier,
        spread,
        sqbuf,
        opm,
        gated,
        active,
        psend,
        precv,
        csend,
        crecv,
        own,
        sbuf,
        scale,
        send_sem,
        recv_sem,
        load_sem,
    ) = rest
    (
        x_ref, gain1_ref, wprod_ref, sprod_ref, wplace_ref, splace_ref, gains_ref, op_ref, bias_ref,
        wblend_ref, sblend_ref, gain2_ref, wsw_ref, ssw_ref, wex_ref, sex_ref, wcon_ref, scon_ref,
    ) = local
    rep, fs, tp = lax.axis_index("rep"), lax.axis_index("fs"), lax.axis_index("tp")
    zl, y = fs // NY, lax.rem(fs, NY)
    x, core = tp // 2, lax.rem(tp, 2)
    z = rep * NZ + zl

    def at_z(d):
        zz = lax.rem(z + d + NREP * NZ, NREP * NZ)
        return {"rep": zz // NZ, "fs": lax.rem(zz, NZ) * NY + y}

    def at_y(d):
        return {"fs": zl * NY + lax.rem(y + d + NY, NY)}

    def at_tp(k):
        return {"tp": lax.rem(tp + k + NTP, NTP)}

    def at_x(k):
        return {"tp": lax.rem(x + k + NX, NX) * 2 + core}

    partner = {"tp": x * 2 + 1 - core}

    def slot(a):
        return lax.rem(zl - a[0] + NZ, NZ) * NY + lax.rem(y - a[1] + NY, NY)

    def send(key, src, dst, dev):
        pltpu.make_async_remote_copy(
            src_ref=src, dst_ref=dst, send_sem=send_sem.at[KINDS.index(key[0])], recv_sem=recv_sem.at[plan.copies[key]],
            device_id=dev, device_id_type=MESH,
        ).start()

    def arrive(key, dst, dev):
        pltpu.make_async_remote_copy(
            src_ref=dst, dst_ref=dst, send_sem=send_sem.at[KINDS.index(key[0])], recv_sem=recv_sem.at[plan.copies[key]],
            device_id=dev, device_id_type=MESH,
        ).wait_recv()

    arrs = [arrivals_of(s) for s in STREAMS]

    def block(s, a):
        return g.at[slot(a), pl.ds(STREAMS[s][0], STREAMS[s][1])]

    def forward(s, a):
        for b, (parent, axis, step) in arrs[s].items():
            if parent == a:
                send(("w", s, *b), block(s, a), block(s, a), at_z(step) if axis == "z" else at_y(step))

    zs = sorted({e * v[2] for a in arrs for v in a.values() if v[1] == "z" for e in (1, -1)})
    ys = sorted({(e * v[2]) % NY for a in arrs for v in a.values() if v[1] == "y" for e in (1, -1)})
    greet = [at_z(d) for d in zs] + [at_y(d) for d in ys] + [at_tp(k) for k in range(1, NTP)]
    barrier = pltpu.get_barrier_semaphore()
    for dev in greet:
        pl.semaphore_signal(barrier, inc=1, device_id=dev, device_id_type=MESH)

    def loading(name):
        i = NAMES.index(name)
        return pltpu.make_async_copy(hbm[i], local[i], load_sem.at[i])

    for name in LOADS:
        loading(name).start()

    def load(*names):
        for name in names:
            loading(name).wait()

    def pack1():
        load("wprod", "wplace", "wblend", "sblend")
        g[fs, R_PROD : R_PROD + 64, :] = wprod_ref[...].astype(BF16)
        g[fs, R_PLACE : R_PLACE + 64, :] = wplace_ref[...].astype(BF16)
        wb = wblend_ref[...].astype(BF16).astype(F32) * jnp.broadcast_to(sblend_ref[...], (128, 64)).T
        g[fs, R_BLEND : R_BLEND + 64, :] = wb.astype(BF16)
        pl.semaphore_wait(barrier, len(greet))

    def pack2():
        load("wsw", "wex", "ssw", "sex")
        for i, w in ((0, wsw_ref), (2, wex_ref)):
            for j in (0, 1):
                g[fs, R_SE + 64 * (i + j) : R_SE + 64 * (i + j + 1), :] = w[:, 128 * j : 128 * (j + 1)].astype(BF16)
        zero = jnp.zeros((64, 128), BF16)
        for i, w in ((4, wsw_ref), (5, wex_ref)):
            g[fs, R_SE + 64 * i : R_SE + 64 * (i + 1), :] = zero
            g[fs, R_SE + 64 * i : R_SE + 64 * (i + 1), 0:96] = w[:, 256:352].astype(BF16)
        scale[...] = jnp.zeros_like(scale)
        scale[0:1, 0:HID] = ssw_ref[...].reshape(1, HID)
        scale[1:2, 0:HID] = sex_ref[...].reshape(1, HID)

    def pack3():
        load("wcon", "scon")
        by = jnp.broadcast_to(scon_ref[...], (128, 64)).T[:, 0:1]
        wc = (wcon_ref[...].astype(BF16).astype(F32) * by).astype(BF16)
        g[fs, R_CON : R_CON + 64, :] = wc[:, 0:128]
        g[fs, R_CON + 64 : R_CON + 128, :] = wc[:, 128:256]
        g[fs, R_CON + 128 : R_CON + 192, :] = jnp.zeros((64, 128), BF16)
        g[fs, R_CON + 128 : R_CON + 192, 0:96] = wc[:, 256:352]

    def go(s):
        forward(s, (0, 0))

    def recv(s, dz, dy):
        _, axis, step = arrs[s][(dz, dy)]
        arrive(("w", s, dz, dy), block(s, (dz, dy)), at_z(-step) if axis == "z" else at_y(-step))
        forward(s, (dz, dy))

    def leaf(s):
        leaves = leaves_of(arrs[s])
        ref = g.at[0 : len(leaves), pl.ds(STREAMS[s][0], STREAMS[s][1])]
        arrive(("w", s, *leaves[0]), ref, at_y(1))

    def tile(row):
        return g[:, row : row + 64, :].reshape(DIM, 128)

    def norm():
        load("x", "gain1")
        v = x_ref[...].astype(F32)
        r = lax.rsqrt(jnp.mean(v * v, axis=-1, keepdims=True) + EPS)
        normed[...] = (v * r * gain1_ref[...]).astype(BF16)

    def enter():
        load("sprod", "splace")
        w = jnp.concatenate([tile(R_PROD), tile(R_PLACE)], axis=1)
        h = jnp.dot(normed[...], w, preferred_element_type=F32)
        sp = jax.nn.gelu(h[:, 128:256] * splace_ref[...])
        spread[...] = sp
        sqbuf[tp] = jnp.sum((sp * sp).T, axis=0, keepdims=True)
        for k in range(1, NTP):
            send(("sq", k), sqbuf.at[tp], sqbuf.at[tp], at_tp(k))
        carrier[...] = jax.nn.gelu(h[:, 0:128] * sprod_ref[...])

    def mask():
        load("op", "gains", "bias", "gain2")
        t = lax.broadcasted_iota(jnp.int32, (BLOCK, BLOCK), 0)
        s = lax.broadcasted_iota(jnp.int32, (BLOCK, BLOCK), 1)
        opm[...] = jnp.where(t >= s, op_ref[tp].astype(F32), 0.0).astype(BF16)

    def mixed():
        for k in range(1, NTP):
            src = lax.rem(tp - k + NTP, NTP)
            arrive(("sq", k), sqbuf.at[src], at_tp(-k))
        total = jnp.sum(sqbuf[...], axis=0)
        r = lax.rsqrt(total / CH + EPS)
        r = jnp.broadcast_to(r, (128, TOK)).T
        sn = (spread[...] * r * gains_ref[...]).astype(BF16)
        bias = jnp.broadcast_to(bias_ref[pl.ds(tp, 1), :], (BLOCK, BLOCK)).T
        w = opm[...]
        for n in range(TOK // BLOCK):
            rows = slice(n * BLOCK, (n + 1) * BLOCK)
            m = jnp.dot(w, sn[rows], preferred_element_type=F32) + bias
            gated[rows, :] = (carrier[rows, :] * m).astype(BF16)

    nt = (((1,), (1,)), ((), ()))

    def product(w, d, r=slice(None)):
        if w == 0:
            b = g[pl.ds(4 * d, 4), R_BLEND : R_BLEND + 64, :].reshape(256, 128)
            return lax.dot_general(gated[r, :], b, nt, preferred_element_type=F32)
        cols = [g[pl.ds(4 * d, 4), R_CON + 64 * j : R_CON + 64 * (j + 1), :].reshape(256, 128) for j in range(3)]
        return lax.dot_general(active[r, :], jnp.concatenate(cols, axis=1), nt, preferred_element_type=F32)

    def chip(k):
        return lax.rem(x + k, NX) * 2

    def part(w, k):
        psend[w, k] = product(w, chip(k) + 1 - core).astype(BF16)
        send(("p", w, k), psend.at[w, k], precv.at[w, k], partner)

    def rows(h):
        return slice(128 * h, 128 * (h + 1))

    def sum2(w):
        v = product(w, chip(2) + core)
        arrive(("p", w, 2), precv.at[w, 2], partner)
        csend[w, 0] = (v + precv[w, 2].astype(F32)).astype(BF16)
        for h in (0, 1):
            send(("c", w, 2, h), csend.at[w, 0, rows(h)], crecv.at[w, 0, rows(h)], at_x(-1 if h else 1))

    def add(w, k, h):
        v = product(w, chip(k) + core, rows(h))
        if (k, h) in ((1, 1), (3, 0)):
            arrive(("p", w, k), precv.at[w, k], partner)
        v = v + precv[w, k, rows(h)].astype(F32)
        if (k, h) in ((1, 0), (3, 1)):
            arrive(("c", w, 2, h), crecv.at[w, 0, rows(h)], at_x(1 if h else -1))
            v = v + crecv[w, 0, rows(h)].astype(F32)
        i = 1 if k == 1 else 2
        csend[w, i, rows(h)] = v.astype(BF16)
        send(("c", w, k, h), csend.at[w, i, rows(h)], crecv.at[w, i, rows(h)], at_x(k))

    def keep(w):
        v = product(w, chip(0) + core)
        arrive(("p", w, 0), precv.at[w, 0], partner)
        own[...] = v + precv[w, 0].astype(F32)

    def total(w):
        v = own[...]
        for k in (1, 3):
            i = 1 if k == 1 else 2
            for h in (0, 1):
                arrive(("c", w, k, h), crecv.at[w, i, rows(h)], at_x(-k))
            v = v + crecv[w, i].astype(F32)
        return v

    def stream():
        mine = x_ref[:, pl.ds(pl.multiple_of(tp * 256, 256), 256)].astype(F32)
        sbuf[tp] = (mine + total(0)).astype(BF16)
        for k, h in ((1, 0), (3, 1), (1, 1), (3, 0)):
            send(("ac", k, h), sbuf.at[tp, rows(h)], sbuf.at[tp, rows(h)], at_x(k))
        send(("ap", 0, 0), sbuf.at[tp], sbuf.at[tp], partner)

    def relay(k, h):
        d = lax.rem(x - k + NX, NX) * 2 + core
        ref = sbuf.at[d, rows(h)]
        arrive(("ac", k, h), ref, at_x(-k) if k != 2 else at_x(1 if h else -1))
        if (k, h) in ((1, 0), (3, 1)):
            send(("ac", 2, h), ref, ref, at_x(-1 if h else 1))
        send(("ap", k, h), ref, ref, partner)

    def norm2():
        for k in range(4):
            d = lax.rem(x - k + NX, NX) * 2 + 1 - core
            if k == 0:
                arrive(("ap", 0, 0), sbuf.at[d], partner)
            else:
                for h in (0, 1):
                    arrive(("ap", k, h), sbuf.at[d, rows(h)], partner)
        sq = jnp.zeros((TOK, 256), F32)
        for d in range(NTP):
            v = sbuf[d].astype(F32)
            sq = sq + v * v
        r = lax.rsqrt(jnp.sum(sq, axis=-1, keepdims=True) / DIM + EPS)
        for d in range(NTP):
            cols = slice(256 * d, 256 * (d + 1))
            normed[:, cols] = (sbuf[d].astype(F32) * r * gain2_ref[:, cols]).astype(BF16)

    def hidden():
        for j, (a, b) in enumerate(((0, 2), (1, 3), (4, 5))):
            w = jnp.concatenate([tile(R_SE + 64 * a), tile(R_SE + 64 * b)], axis=1)
            h = jnp.dot(normed[...], w, preferred_element_type=F32)
            cols = slice(128 * j, 128 * (j + 1))
            gate = h[:, 0:128] * scale[0:1, cols]
            up = h[:, 128:256] * scale[1:2, cols]
            active[:, cols] = (gate / (1.0 + jnp.exp(-gate)) * up).astype(BF16)

    def out():
        out_ref[...] = (sbuf[tp].astype(F32) + total(1)).astype(BF16)

    run = {
        "pack1": pack1, "pack2": pack2, "pack3": pack3, "go": go, "norm": norm, "in": enter, "mask": mask, "mixed": mixed, "stream": stream,
        "norm2": norm2, "hidden": hidden, "out": out, "recv": recv, "leaf": leaf, "part": part, "sum": add, "sum2": sum2, "own": keep, "pass": relay,
    }
    for key, _ in seq:
        if isinstance(key, tuple):
            run[key[0]](*key[1:])
        else:
            run[key]()
    for i, all_sent in enumerate((g.at[0:31], sqbuf.at[0:7], psend, csend, sbuf.at[0:3], sbuf.at[0:4])):
        pltpu.make_async_copy(all_sent, all_sent, send_sem.at[i]).wait()


def on_device(*args):
    plan = make_plan()
    seq = plan.order()
    n = len(plan.groups)
    args = list(args)
    for i in (NAMES.index("wblend"), NAMES.index("wcon")):
        args[i] = args[i].T
    args = [a.reshape(1, -1) if a.ndim == 1 and a.size != HID else a for a in args]
    return pl.pallas_call(
        functools.partial(kernel, plan, seq),
        out_shape=jax.ShapeDtypeStruct((TOK, 256), BF16),
        in_specs=[pl.BlockSpec(memory_space=pltpu.HBM)] * len(args),
        out_specs=pl.BlockSpec(memory_space=pltpu.VMEM),
        scratch_shapes=[
            *[pltpu.VMEM(a.shape, a.dtype) for a in args],
            pltpu.VMEM((NY * NZ, R_ALL, 128), BF16),
            pltpu.VMEM((TOK, DIM), BF16),
            pltpu.VMEM((TOK, 128), F32),
            pltpu.VMEM((TOK, 128), F32),
            pltpu.VMEM((NTP, 1, TOK), F32),
            pltpu.VMEM((BLOCK, BLOCK), BF16),
            pltpu.VMEM((TOK, 128), BF16),
            pltpu.VMEM((TOK, 384), BF16),
            pltpu.VMEM((2, 4, TOK, 256), BF16),
            pltpu.VMEM((2, 4, TOK, 256), BF16),
            pltpu.VMEM((2, 3, TOK, 256), BF16),
            pltpu.VMEM((2, 3, TOK, 256), BF16),
            pltpu.VMEM((TOK, 256), F32),
            pltpu.VMEM((NTP, TOK, 256), BF16),
            pltpu.VMEM((8, 384), F32),
            pltpu.SemaphoreType.DMA((len(KINDS),)),
            pltpu.SemaphoreType.DMA((n,)),
            pltpu.SemaphoreType.DMA((len(args),)),
        ],
        compiler_params=pltpu.CompilerParams(
            collective_id=0, has_side_effects=True, vmem_limit_bytes=67043328
        ),
        name="layer",
    )(*args)


def solution(mesh):
    return jax.shard_map(
        on_device,
        mesh=mesh,
        in_specs=(
            P(("rep", "fs"), None),
            P(),
            P("fs", "tp"),
            P("tp"),
            P("fs", "tp"),
            P("tp"),
            P("tp"),
            P(),
            P(),
            P("tp", "fs"),
            P("fs"),
            P(),
            P("fs", "tp"),
            P("tp"),
            P("fs", "tp"),
            P("tp"),
            P("tp", "fs"),
            P("fs"),
        ),
        out_specs=P(("rep", "fs"), "tp"),
        check_vma=False,
    )
```

```python
import functools

import jax
import jax.numpy as jnp
from jax import lax
from jax.experimental import pallas as pl
from jax.experimental.pallas import tpu as pltpu
from jax.sharding import PartitionSpec as P

EPS = 1e-06
F32 = jnp.float32
BF16 = jnp.bfloat16
MESH = pl.DeviceIdType.MESH

TOK = 256
BLOCK = 128
DIM = 2048
CH = 1024
HID = 352
NY, NZ, NX, NTP, NREP = 4, 8, 4, 8, 4

R_PROD, R_PLACE, R_BLEND, R_SE, R_CON, R_ALL = 0, 64, 128, 192, 576, 720
R_TAIL = R_SE + 256

RING4 = {1: 0, 2: 1, 3: 2, 4: 3, -1: 0, -2: -1, -3: -2}
RING3 = {1: 0, 2: 1, 3: 2, -1: 0, -2: -1, -3: -2, -4: -3}
JUMP4 = {1: 0, 2: 0, 3: 2, 4: 2, -1: 0, -2: 0, -3: -2}
JUMP3 = {1: 0, 2: 0, 3: 2, -1: 0, -2: 0, -3: -2, -4: -2}
FAR4 = {1: 0, 2: 0, 3: 0, 4: 0, -1: 0, -2: 0, -3: 0}
FAR3 = {1: 0, 2: 0, 3: 0, -1: 0, -2: 0, -3: 0, -4: 0}
YUP = {1: 0, -1: 0, 2: 1}
YDN = {1: 0, -1: 0, -2: -1}
YUP2 = {1: 0, -1: 0, 2: 0}
YDN2 = {1: 0, -1: 0, -2: 0}

KINDS = ("w", "sq", "p", "c", "ac", "ap")
NAMES = (
    "x", "gain1", "wprod", "sprod", "wplace", "splace", "gains", "op", "bias",
    "wblend", "sblend", "gain2", "wsw", "ssw", "wex", "sex", "wcon", "scon",
)
LOADS = (
    "wprod", "wplace", "wblend", "sblend", "wsw", "wex", "wcon", "scon", "x", "gain1", "sprod", "splace",
    "op", "gains", "bias", "ssw", "sex", "gain2",
)

STREAMS = (
    (0, 64, "z", JUMP3, YDN, 0.0, 1.0),
    (64, 64, "y", JUMP4, YUP, 0.0, 0.5),
    (128, 64, "z", JUMP3, YDN, 0.0, 0.5),
    (192, 192, "z", RING4, YUP, 8.6, 1.0),
    (384, 192, "y", RING4, YUP, 12.7, 1.0),
    (576, 144, "z", JUMP3, YDN, 14.4, 2.0),
)
IN, BLEND, SE, CON = (0, 1), (2,), (3, 4), (5,)


def order_of(tree):
    return sorted(tree, key=lambda d: (abs(d), -d))


def arrivals_of(stream):
    first, zt, yt = stream[2:5]
    out = {}
    if first == "z":
        for dz in order_of(zt):
            out[(dz, 0)] = ((zt[dz], 0), "z", dz - zt[dz])
        for dz in [0, *order_of(zt)]:
            for dy in order_of(yt):
                out[(dz, dy)] = ((dz, yt[dy]), "y", dy - yt[dy])
    else:
        for dy in order_of(yt):
            out[(0, dy)] = ((0, yt[dy]), "y", dy - yt[dy])
        for dy in [0, *order_of(yt)]:
            for dz in order_of(zt):
                out[(dz, dy)] = ((zt[dz], dy), "z", dz - zt[dz])
    return out


def leaves_of(arrivals):
    parents = {v[0] for v in arrivals.values()}
    return [a for a in arrivals if a not in parents]


LATENCY = {"d2d": 0.6, "q": 2.9, "z+": 1.05, "z-": 1.05, "y+": 1.05, "y-": 1.05, "x+": 1.25, "x-": 1.25}


class Plan:
    def __init__(self):
        self.tasks = {}
        self.copies = {}
        self.groups = {}

    def copy(self, key, link, size, hops, group=None):
        self.copies[key] = self.groups.setdefault(group or key, len(self.groups))
        return (key, link, size, hops)

    def task(self, key, deps, dur, sends=(), rank=1, begin=0.0, slack=0.0):
        self.tasks[key] = (tuple(deps), dur, tuple(sends), rank, begin, slack)

    def order(self):
        t, arrived, free, done, seq = 0.0, {}, {}, {}, []
        waits = {k: sum(1 for _ in v[0]) for k, v in self.tasks.items()}
        users, ready, open_ = {}, {k: v[4] for k, v in self.tasks.items()}, set()
        for k, v in self.tasks.items():
            for d in v[0]:
                users.setdefault(d, []).append(k)
            if not waits[k]:
                open_.add(k)

        def came(d, at):
            for k in users.get(d, ()):
                waits[k] -= 1
                ready[k] = max(ready[k], at + (self.tasks[k][5] if d not in self.tasks else 0.0))
                if not waits[k]:
                    open_.add(k)

        index = {k: i for i, k in enumerate(self.tasks)}
        while open_:
            best = min(open_, key=lambda k: (max(ready[k], t), self.tasks[k][3], ready[k], index[k]))
            open_.remove(best)
            _, dur, sends, *_ = self.tasks[best]
            t = max(t, ready[best]) + dur
            came(best, t)
            for key, link, size, hops in sends:
                rate = 650e3 if link == "d2d" else 45e3
                begin = max(free.get(link, 0.0), t)
                wire = size * max(hops, 1) / rate
                free[link] = begin + wire
                came(key, begin + wire + LATENCY.get(link, 0.5) + 0.75 * hops)
            seq.append((best, t))
        assert len(seq) == len(self.tasks)
        return seq


def make_plan():
    plan = Plan()
    stream_tasks = {}
    plan.task("pack1", [], 1.5)
    plan.task("pack2", ["pack1"], 0.3, (), 2)
    for s, stream in enumerate(STREAMS):
        arr = arrivals_of(stream)
        leaves = leaves_of(arr)
        sends = {}
        for a, (parent, axis, step) in arr.items():
            key = ("w", s, *a)
            link = axis + ("+" if step > 0 else "-")
            cp = plan.copy(key, link, stream[1] * 256, abs(step), ("leaf", s) if a in leaves else key)
            sends.setdefault(parent, []).append(cp)
        pack = "pack1" if s in IN + BLEND else "pack2"
        plan.task(("go", s), [pack], 0.03, sends[(0, 0)], 0, stream[5])
        for a in arr:
            if a not in leaves:
                plan.task(("recv", s, *a), [("w", s, *a), ("go", s)], 0.03, sends[a], 0, 0.0, stream[6])
        plan.task(("leaf", s), [("go", s), *[("w", s, *a) for a in leaves]], 0.03, (), 1)
        stream_tasks[s] = [("recv", s, *a) for a in arr if a not in leaves] + [("leaf", s)]

    def whole(which):
        return [t for s in which for t in stream_tasks[s]]

    plan.task("norm", ["pack1"], 0.45, (), 2)
    sq = [plan.copy(("sq", k), "d2d" if k == 4 else "q", 1024, 1) for k in range(1, NTP)]
    plan.task("spread", ["norm", *whole(IN[1:])], 0.6, sq, 1)
    plan.task("carrier", ["norm", *whole(IN[:1])], 0.5, (), 2)
    plan.task("mask", ["pack1"], 0.03, (), 3)
    plan.task("mixed", ["spread", "carrier", "mask", *[("sq", k) for k in range(1, NTP)]], 0.45, (), 1)

    half = 65536

    def scatter(w, deps, dur):
        last = deps
        for k in (2, 1, 3, 0):
            cp = plan.copy(("p", w, k), "d2d", 2 * half, 1)
            plan.task(("part", w, k), last, dur, (cp,), 1)
            last = [("part", w, k)]
        cps = [plan.copy(("c", w, 2, h), "x-" if h else "x+", half, 1) for h in (0, 1)]
        plan.task(("sum2", w), [("part", w, 2), ("p", w, 2)], dur + 0.1, cps, 1)
        for k, h in ((1, 1), (3, 0), (1, 0), (3, 1)):
            cp = plan.copy(("c", w, k, h), "x-" if k == 3 else "x+", half, 1)
            need = [("c", w, 2, h), ("sum", w, k, 1 - h)] if (k, h) in ((1, 0), (3, 1)) else [("sum2", w)]
            plan.task(("sum", w, k, h), [("part", w, k), *need, ("p", w, k)], dur * 0.6 + 0.1, (cp,), 1)
        plan.task(("own", w), [("part", w, 0), ("p", w, 0)], dur, (), 2)
        return [("own", w)] + [("c", w, k, h) for k in (1, 3) for h in (0, 1)]

    after = scatter(0, ["mixed", *whole(BLEND)], 0.2)
    ag = [plan.copy(("ac", k, h), "x-" if k == 3 else "x+", half, 1) for k, h in ((1, 0), (3, 1), (1, 1), (3, 0))]
    ag.append(plan.copy(("ap", 0, 0), "d2d", 2 * half, 1))
    plan.task("stream", after, 0.2, ag, 1)
    got = [("ap", 0, 0)]
    for k, h in ((1, 0), (3, 1), (1, 1), (3, 0), (2, 0), (2, 1)):
        cps = []
        if (k, h) in ((1, 0), (3, 1)):
            cps.append(plan.copy(("ac", 2, h), "x-" if h else "x+", half, 1))
        cps.append(plan.copy(("ap", k, h), "d2d", half, 1))
        plan.task(("pass", k, h), [("ac", k, h), "stream"], 0.03, cps, 0)
        got += [("pass", k, h), ("ap", k, h)]
    plan.task("norm2", ["stream", *got], 0.5, (), 1)
    plan.task("hidden", ["norm2", *whole(SE)], 1.3, (), 1)
    plan.task("unpack", [*whole(SE[-1:]), *whole(CON)], 0.5, (), 1)
    after = scatter(1, ["hidden", "unpack"], 0.3)
    plan.task("out", after, 0.3, (), 1)
    return plan


def kernel(
    plan,
    seq,
    *refs,
):
    hbm, out_ref, rest = refs[: len(NAMES)], refs[len(NAMES)], refs[len(NAMES) + 1 :]
    local, rest = rest[: len(NAMES)], rest[len(NAMES) :]
    (
        g,
        normed,
        carrier,
        spread,
        tail,
        sqbuf,
        opm,
        gated,
        active,
        psend,
        precv,
        csend,
        crecv,
        own,
        sbuf,
        scale,
        send_sem,
        recv_sem,
        load_sem,
    ) = rest
    (
        x_ref, gain1_ref, wprod_ref, sprod_ref, wplace_ref, splace_ref, gains_ref, op_ref, bias_ref,
        wblend_ref, sblend_ref, gain2_ref, wsw_ref, ssw_ref, wex_ref, sex_ref, wcon_ref, scon_ref,
    ) = local
    rep, fs, tp = lax.axis_index("rep"), lax.axis_index("fs"), lax.axis_index("tp")
    zl, y = fs // NY, lax.rem(fs, NY)
    x, core = tp // 2, lax.rem(tp, 2)
    z = rep * NZ + zl

    def at_z(d):
        zz = lax.rem(z + d + NREP * NZ, NREP * NZ)
        return {"rep": zz // NZ, "fs": lax.rem(zz, NZ) * NY + y}

    def at_y(d):
        return {"fs": zl * NY + lax.rem(y + d + NY, NY)}

    def at_tp(k):
        return {"tp": lax.rem(tp + k + NTP, NTP)}

    def at_x(k):
        return {"tp": lax.rem(x + k + NX, NX) * 2 + core}

    partner = {"tp": x * 2 + 1 - core}

    def slot(a):
        return lax.rem(zl - a[0] + NZ, NZ) * NY + lax.rem(y - a[1] + NY, NY)

    def send(key, src, dst, dev):
        pltpu.make_async_remote_copy(
            src_ref=src, dst_ref=dst, send_sem=send_sem.at[KINDS.index(key[0])], recv_sem=recv_sem.at[plan.copies[key]],
            device_id=dev, device_id_type=MESH,
        ).start()

    def arrive(key, dst, dev):
        pltpu.make_async_remote_copy(
            src_ref=dst, dst_ref=dst, send_sem=send_sem.at[KINDS.index(key[0])], recv_sem=recv_sem.at[plan.copies[key]],
            device_id=dev, device_id_type=MESH,
        ).wait_recv()

    arrs = [arrivals_of(s) for s in STREAMS]

    def block(s, a):
        return g.at[slot(a), pl.ds(STREAMS[s][0], STREAMS[s][1])]

    def forward(s, a):
        for b, (parent, axis, step) in arrs[s].items():
            if parent == a:
                send(("w", s, *b), block(s, a), block(s, a), at_z(step) if axis == "z" else at_y(step))

    zs = sorted({e * v[2] for a in arrs for v in a.values() if v[1] == "z" for e in (1, -1)})
    ys = sorted({(e * v[2]) % NY for a in arrs for v in a.values() if v[1] == "y" for e in (1, -1)})
    greet = [at_z(d) for d in zs] + [at_y(d) for d in ys] + [at_tp(k) for k in range(1, NTP)]
    barrier = pltpu.get_barrier_semaphore()
    for dev in greet:
        pl.semaphore_signal(barrier, inc=1, device_id=dev, device_id_type=MESH)

    def loading(name):
        i = NAMES.index(name)
        return pltpu.make_async_copy(hbm[i], local[i], load_sem.at[i])

    for name in LOADS:
        loading(name).start()

    def load(*names):
        for name in names:
            loading(name).wait()

    def pack1():
        load("wprod", "wplace", "wblend", "sblend")
        g[fs, R_PROD : R_PROD + 64, :] = wprod_ref[...].astype(BF16)
        g[fs, R_PLACE : R_PLACE + 64, :] = wplace_ref[...].astype(BF16)
        wb = wblend_ref[...].astype(BF16).astype(F32) * jnp.broadcast_to(sblend_ref[...], (128, 64)).T
        g[fs, R_BLEND : R_BLEND + 64, :] = wb.astype(BF16)
        pl.semaphore_wait(barrier, len(greet))

    def pack2():
        load("wsw", "wex", "ssw", "sex")
        for i, w in ((0, wsw_ref), (2, wex_ref)):
            for j in (0, 1):
                g[fs, R_SE + 64 * (i + j) : R_SE + 64 * (i + j + 1), :] = w[:, 128 * j : 128 * (j + 1)].astype(BF16)
        load("wcon", "scon")
        by = jnp.broadcast_to(scon_ref[...], (128, 64)).T[:, 0:1]
        wc = (wcon_ref[...].astype(BF16).astype(F32) * by).astype(BF16)
        for i, w in ((0, wsw_ref), (1, wex_ref)):
            at = pl.ds(R_TAIL + 64 * i, 64)
            g[fs, at, 0:96] = w[:, 256:352].astype(BF16)
            g[fs, at, 96:128] = wc[:, 256 + 32 * i : 288 + 32 * i]
        g[fs, R_CON : R_CON + 64, :] = wc[:, 0:128]
        g[fs, R_CON + 64 : R_CON + 128, :] = wc[:, 128:256]
        for q in range(4):
            g[fs, R_CON + 128 : R_CON + 144, 32 * q : 32 * (q + 1)] = wc[16 * q : 16 * (q + 1), 320:352]
        scale[...] = jnp.zeros_like(scale)
        scale[0:1, 0:HID] = ssw_ref[...].reshape(1, HID)
        scale[1:2, 0:HID] = sex_ref[...].reshape(1, HID)

    def unpack():
        for i in (0, 1):
            tail[:, :, 32 * i : 32 * (i + 1)] = g[:, R_TAIL + 64 * i : R_TAIL + 64 * (i + 1), 96:128]
        for q in range(4):
            tail[:, 16 * q : 16 * (q + 1), 64:96] = g[:, R_CON + 128 : R_CON + 144, 32 * q : 32 * (q + 1)]

    def go(s):
        forward(s, (0, 0))

    def recv(s, dz, dy):
        _, axis, step = arrs[s][(dz, dy)]
        arrive(("w", s, dz, dy), block(s, (dz, dy)), at_z(-step) if axis == "z" else at_y(-step))
        forward(s, (dz, dy))

    def leaf(s):
        leaves = leaves_of(arrs[s])
        ref = g.at[0 : len(leaves), pl.ds(STREAMS[s][0], STREAMS[s][1])]
        arrive(("w", s, *leaves[0]), ref, at_y(1))

    def tile(row):
        return g[:, row : row + 64, :].reshape(DIM, 128)

    def norm():
        load("x", "gain1")
        v = x_ref[...].astype(F32)
        r = lax.rsqrt(jnp.mean(v * v, axis=-1, keepdims=True) + EPS)
        normed[...] = (v * r * gain1_ref[...]).astype(BF16)

    def spreading():
        load("splace")
        h = jnp.dot(normed[...], tile(R_PLACE), preferred_element_type=F32)
        sp = jax.nn.gelu(h * splace_ref[...])
        spread[...] = sp
        sqbuf[tp] = jnp.sum((sp * sp).T, axis=0, keepdims=True)
        for k in range(1, NTP):
            send(("sq", k), sqbuf.at[tp], sqbuf.at[tp], at_tp(k))

    def carry():
        load("sprod")
        h = jnp.dot(normed[...], tile(R_PROD), preferred_element_type=F32)
        carrier[...] = jax.nn.gelu(h * sprod_ref[...])

    def mask():
        load("op", "gains", "bias", "gain2")
        tail[...] = jnp.zeros_like(tail)
        t = lax.broadcasted_iota(jnp.int32, (BLOCK, BLOCK), 0)
        s = lax.broadcasted_iota(jnp.int32, (BLOCK, BLOCK), 1)
        opm[...] = jnp.where(t >= s, op_ref[tp].astype(F32), 0.0).astype(BF16)

    def mixed():
        for k in range(1, NTP):
            src = lax.rem(tp - k + NTP, NTP)
            arrive(("sq", k), sqbuf.at[src], at_tp(-k))
        total = jnp.sum(sqbuf[...], axis=0)
        r = lax.rsqrt(total / CH + EPS)
        r = jnp.broadcast_to(r, (128, TOK)).T
        sn = (spread[...] * r * gains_ref[...]).astype(BF16)
        bias = jnp.broadcast_to(bias_ref[pl.ds(tp, 1), :], (BLOCK, BLOCK)).T
        w = opm[...]
        for n in range(TOK // BLOCK):
            rows = slice(n * BLOCK, (n + 1) * BLOCK)
            m = jnp.dot(w, sn[rows], preferred_element_type=F32) + bias
            gated[rows, :] = (carrier[rows, :] * m).astype(BF16)

    nt = (((1,), (1,)), ((), ()))

    def product(w, d, r=slice(None)):
        if w == 0:
            b = g[pl.ds(4 * d, 4), R_BLEND : R_BLEND + 64, :].reshape(256, 128)
            return lax.dot_general(gated[r, :], b, nt, preferred_element_type=F32)
        cols = [g[pl.ds(4 * d, 4), R_CON + 64 * j : R_CON + 64 * (j + 1), :].reshape(256, 128) for j in (0, 1)]
        cols.append(tail[pl.ds(4 * d, 4)].reshape(256, 128))
        return lax.dot_general(active[r, :], jnp.concatenate(cols, axis=1), nt, preferred_element_type=F32)

    def chip(k):
        return lax.rem(x + k, NX) * 2

    def part(w, k):
        psend[w, k] = product(w, chip(k) + 1 - core).astype(BF16)
        send(("p", w, k), psend.at[w, k], precv.at[w, k], partner)

    def rows(h):
        return slice(128 * h, 128 * (h + 1))

    def sum2(w):
        v = product(w, chip(2) + core)
        arrive(("p", w, 2), precv.at[w, 2], partner)
        csend[w, 0] = (v + precv[w, 2].astype(F32)).astype(BF16)
        for h in (0, 1):
            send(("c", w, 2, h), csend.at[w, 0, rows(h)], crecv.at[w, 0, rows(h)], at_x(-1 if h else 1))

    def add(w, k, h):
        v = product(w, chip(k) + core, rows(h))
        if (k, h) in ((1, 1), (3, 0)):
            arrive(("p", w, k), precv.at[w, k], partner)
        v = v + precv[w, k, rows(h)].astype(F32)
        if (k, h) in ((1, 0), (3, 1)):
            arrive(("c", w, 2, h), crecv.at[w, 0, rows(h)], at_x(1 if h else -1))
            v = v + crecv[w, 0, rows(h)].astype(F32)
        i = 1 if k == 1 else 2
        csend[w, i, rows(h)] = v.astype(BF16)
        send(("c", w, k, h), csend.at[w, i, rows(h)], crecv.at[w, i, rows(h)], at_x(k))

    def keep(w):
        v = product(w, chip(0) + core)
        arrive(("p", w, 0), precv.at[w, 0], partner)
        own[...] = v + precv[w, 0].astype(F32)

    def total(w):
        v = own[...]
        for k in (1, 3):
            i = 1 if k == 1 else 2
            for h in (0, 1):
                arrive(("c", w, k, h), crecv.at[w, i, rows(h)], at_x(-k))
            v = v + crecv[w, i].astype(F32)
        return v

    def stream():
        mine = x_ref[:, pl.ds(pl.multiple_of(tp * 256, 256), 256)].astype(F32)
        sbuf[tp] = (mine + total(0)).astype(BF16)
        for k, h in ((1, 0), (3, 1), (1, 1), (3, 0)):
            send(("ac", k, h), sbuf.at[tp, rows(h)], sbuf.at[tp, rows(h)], at_x(k))
        send(("ap", 0, 0), sbuf.at[tp], sbuf.at[tp], partner)

    def relay(k, h):
        d = lax.rem(x - k + NX, NX) * 2 + core
        ref = sbuf.at[d, rows(h)]
        arrive(("ac", k, h), ref, at_x(-k) if k != 2 else at_x(1 if h else -1))
        if (k, h) in ((1, 0), (3, 1)):
            send(("ac", 2, h), ref, ref, at_x(-1 if h else 1))
        send(("ap", k, h), ref, ref, partner)

    def norm2():
        for k in range(4):
            d = lax.rem(x - k + NX, NX) * 2 + 1 - core
            if k == 0:
                arrive(("ap", 0, 0), sbuf.at[d], partner)
            else:
                for h in (0, 1):
                    arrive(("ap", k, h), sbuf.at[d, rows(h)], partner)
        sq = jnp.zeros((TOK, 256), F32)
        for d in range(NTP):
            v = sbuf[d].astype(F32)
            sq = sq + v * v
        r = lax.rsqrt(jnp.sum(sq, axis=-1, keepdims=True) / DIM + EPS)
        for d in range(NTP):
            cols = slice(256 * d, 256 * (d + 1))
            normed[:, cols] = (sbuf[d].astype(F32) * r * gain2_ref[:, cols]).astype(BF16)

    def hidden():
        for j, (a, b) in enumerate(((0, 2), (1, 3), (4, 5))):
            w = jnp.concatenate([tile(R_SE + 64 * a), tile(R_SE + 64 * b)], axis=1)
            h = jnp.dot(normed[...], w, preferred_element_type=F32)
            cols = slice(128 * j, 128 * (j + 1))
            gate = h[:, 0:128] * scale[0:1, cols]
            up = h[:, 128:256] * scale[1:2, cols]
            active[:, cols] = (gate / (1.0 + jnp.exp(-gate)) * up).astype(BF16)

    def out():
        out_ref[...] = (sbuf[tp].astype(F32) + total(1)).astype(BF16)

    run = {
        "pack1": pack1, "pack2": pack2, "go": go, "norm": norm, "spread": spreading, "carrier": carry, "unpack": unpack, "mask": mask, "mixed": mixed, "stream": stream,
        "norm2": norm2, "hidden": hidden, "out": out, "recv": recv, "leaf": leaf, "part": part, "sum": add, "sum2": sum2, "own": keep, "pass": relay,
    }
    for key, _ in seq:
        if isinstance(key, tuple):
            run[key[0]](*key[1:])
        else:
            run[key]()
    for i, all_sent in enumerate((g.at[0:31], sqbuf.at[0:7], psend, csend, sbuf.at[0:3], sbuf.at[0:4])):
        pltpu.make_async_copy(all_sent, all_sent, send_sem.at[i]).wait()


def on_device(*args):
    plan = make_plan()
    seq = plan.order()
    n = len(plan.groups)
    args = list(args)
    for i in (NAMES.index("wblend"), NAMES.index("wcon")):
        args[i] = args[i].T
    args = [a.reshape(1, -1) if a.ndim == 1 and a.size != HID else a for a in args]
    return pl.pallas_call(
        functools.partial(kernel, plan, seq),
        out_shape=jax.ShapeDtypeStruct((TOK, 256), BF16),
        in_specs=[pl.BlockSpec(memory_space=pltpu.HBM)] * len(args),
        out_specs=pl.BlockSpec(memory_space=pltpu.VMEM),
        scratch_shapes=[
            *[pltpu.VMEM(a.shape, a.dtype) for a in args],
            pltpu.VMEM((NY * NZ, R_ALL, 128), BF16),
            pltpu.VMEM((TOK, DIM), BF16),
            pltpu.VMEM((TOK, 128), F32),
            pltpu.VMEM((TOK, 128), F32),
            pltpu.VMEM((NY * NZ, 64, 128), BF16),
            pltpu.VMEM((NTP, 1, TOK), F32),
            pltpu.VMEM((BLOCK, BLOCK), BF16),
            pltpu.VMEM((TOK, 128), BF16),
            pltpu.VMEM((TOK, 384), BF16),
            pltpu.VMEM((2, 4, TOK, 256), BF16),
            pltpu.VMEM((2, 4, TOK, 256), BF16),
            pltpu.VMEM((2, 3, TOK, 256), BF16),
            pltpu.VMEM((2, 3, TOK, 256), BF16),
            pltpu.VMEM((TOK, 256), F32),
            pltpu.VMEM((NTP, TOK, 256), BF16),
            pltpu.VMEM((8, 384), F32),
            pltpu.SemaphoreType.DMA((len(KINDS),)),
            pltpu.SemaphoreType.DMA((n,)),
            pltpu.SemaphoreType.DMA((len(args),)),
        ],
        compiler_params=pltpu.CompilerParams(
            collective_id=0, has_side_effects=True, vmem_limit_bytes=67043328
        ),
        name="layer",
    )(*args)


def solution(mesh):
    return jax.shard_map(
        on_device,
        mesh=mesh,
        in_specs=(
            P(("rep", "fs"), None),
            P(),
            P("fs", "tp"),
            P("tp"),
            P("fs", "tp"),
            P("tp"),
            P("tp"),
            P(),
            P(),
            P("tp", "fs"),
            P("fs"),
            P(),
            P("fs", "tp"),
            P("tp"),
            P("fs", "tp"),
            P("tp"),
            P("tp", "fs"),
            P("fs"),
        ),
        out_specs=P(("rep", "fs"), "tp"),
        check_vma=False,
    )
```

```python
import functools

import jax
import jax.numpy as jnp
from jax import lax
from jax.experimental import pallas as pl
from jax.experimental.pallas import tpu as pltpu
from jax.sharding import PartitionSpec as P

EPS = 1e-06
F32 = jnp.float32
BF16 = jnp.bfloat16
MESH = pl.DeviceIdType.MESH

TOK = 256
BLOCK = 128
DIM = 2048
CH = 1024
HID = 352
NY, NZ, NX, NTP, NREP = 4, 8, 4, 8, 4

R_PROD, R_PLACE, R_BLEND, R_SE, R_CON, R_ALL = 0, 64, 128, 192, 576, 720
R_TAIL = R_SE + 256

RING4 = {1: 0, 2: 1, 3: 2, 4: 3, -1: 0, -2: -1, -3: -2}
RING3 = {1: 0, 2: 1, 3: 2, -1: 0, -2: -1, -3: -2, -4: -3}
JUMP4 = {1: 0, 2: 0, 3: 2, 4: 2, -1: 0, -2: 0, -3: -2}
JUMP3 = {1: 0, 2: 0, 3: 2, -1: 0, -2: 0, -3: -2, -4: -2}
FAR4 = {1: 0, 2: 0, 3: 0, 4: 0, -1: 0, -2: 0, -3: 0}
FAR3 = {1: 0, 2: 0, 3: 0, -1: 0, -2: 0, -3: 0, -4: 0}
YUP = {1: 0, -1: 0, 2: 1}
YDN = {1: 0, -1: 0, -2: -1}
YUP2 = {1: 0, -1: 0, 2: 0}
YDN2 = {1: 0, -1: 0, -2: 0}

KINDS = ("w", "sq", "p", "c", "ac", "ap")
NAMES = (
    "x", "gain1", "wprod", "sprod", "wplace", "splace", "gains", "op", "bias",
    "wblend", "sblend", "gain2", "wsw", "ssw", "wex", "sex", "wcon", "scon",
)
LOADS = (
    "wprod", "wplace", "wblend", "sblend", "wsw", "wex", "wcon", "scon", "x", "gain1", "sprod", "splace",
    "op", "gains", "bias", "ssw", "sex", "gain2",
)

STREAMS = (
    (0, 64, "z", JUMP3, YDN, 0.0, 1.0),
    (64, 64, "y", JUMP4, YUP, 0.0, 0.5),
    (128, 64, "z", JUMP3, YDN, 0.0, 0.5),
    (192, 192, "z", RING4, YUP, 10.6, 1.0),
    (384, 192, "y", RING4, YUP, 14.7, 1.0),
    (576, 144, "z", JUMP3, YDN, 16.4, 2.0),
)
IN, BLEND, SE, CON = (0, 1), (2,), (3, 4), (5,)


def order_of(tree):
    return sorted(tree, key=lambda d: (abs(d), -d))


def arrivals_of(stream):
    first, zt, yt = stream[2:5]
    out = {}
    if first == "z":
        for dz in order_of(zt):
            out[(dz, 0)] = ((zt[dz], 0), "z", dz - zt[dz])
        for dz in [0, *order_of(zt)]:
            for dy in order_of(yt):
                out[(dz, dy)] = ((dz, yt[dy]), "y", dy - yt[dy])
    else:
        for dy in order_of(yt):
            out[(0, dy)] = ((0, yt[dy]), "y", dy - yt[dy])
        for dy in [0, *order_of(yt)]:
            for dz in order_of(zt):
                out[(dz, dy)] = ((zt[dz], dy), "z", dz - zt[dz])
    return out


def leaves_of(arrivals):
    parents = {v[0] for v in arrivals.values()}
    return [a for a in arrivals if a not in parents]


LATENCY = {"d2d": 0.6, "q": 2.9, "z+": 1.05, "z-": 1.05, "y+": 1.05, "y-": 1.05, "x+": 1.25, "x-": 1.25}


class Plan:
    def __init__(self):
        self.tasks = {}
        self.copies = {}
        self.groups = {}

    def copy(self, key, link, size, hops, group=None):
        self.copies[key] = self.groups.setdefault(group or key, len(self.groups))
        return (key, link, size, hops)

    def task(self, key, deps, dur, sends=(), rank=1, begin=0.0, slack=0.0):
        self.tasks[key] = (tuple(deps), dur, tuple(sends), rank, begin, slack)

    def order(self):
        t, arrived, free, done, seq = 0.0, {}, {}, {}, []
        waits = {k: sum(1 for _ in v[0]) for k, v in self.tasks.items()}
        users, ready, open_ = {}, {k: v[4] for k, v in self.tasks.items()}, set()
        for k, v in self.tasks.items():
            for d in v[0]:
                users.setdefault(d, []).append(k)
            if not waits[k]:
                open_.add(k)

        def came(d, at):
            for k in users.get(d, ()):
                waits[k] -= 1
                ready[k] = max(ready[k], at + (self.tasks[k][5] if d not in self.tasks else 0.0))
                if not waits[k]:
                    open_.add(k)

        index = {k: i for i, k in enumerate(self.tasks)}
        while open_:
            best = min(open_, key=lambda k: (max(ready[k], t), self.tasks[k][3], ready[k], index[k]))
            open_.remove(best)
            _, dur, sends, *_ = self.tasks[best]
            t = max(t, ready[best]) + dur
            came(best, t)
            for key, link, size, hops in sends:
                rate = 650e3 if link == "d2d" else 45e3
                begin = max(free.get(link, 0.0), t)
                wire = size * max(hops, 1) / rate
                free[link] = begin + wire
                came(key, begin + wire + LATENCY.get(link, 0.5) + 0.75 * hops)
            seq.append((best, t))
        assert len(seq) == len(self.tasks)
        return seq


def make_plan():
    plan = Plan()
    stream_tasks = {}
    plan.task("pack1", [], 1.5)
    plan.task("packb", ["pack1"], 0.1, (), 0)
    plan.task("pack2", ["packb"], 0.3, (), 2)
    for s, stream in enumerate(STREAMS):
        arr = arrivals_of(stream)
        leaves = leaves_of(arr)
        sends = {}
        for a, (parent, axis, step) in arr.items():
            key = ("w", s, *a)
            link = axis + ("+" if step > 0 else "-")
            cp = plan.copy(key, link, stream[1] * 256, abs(step), ("leaf", s) if a in leaves else key)
            sends.setdefault(parent, []).append(cp)
        pack = "pack1" if s in IN else "packb" if s in BLEND else "pack2"
        plan.task(("go", s), [pack], 0.03, sends[(0, 0)], 0, stream[5])
        for a in arr:
            if a not in leaves:
                plan.task(("recv", s, *a), [("w", s, *a), ("go", s)], 0.03, sends[a], 0, 0.0, stream[6])
        plan.task(("leaf", s), [("go", s), *[("w", s, *a) for a in leaves]], 0.03, (), 1)
        stream_tasks[s] = [("recv", s, *a) for a in arr if a not in leaves] + [("leaf", s)]

    def whole(which):
        return [t for s in which for t in stream_tasks[s]]

    plan.task("norm", ["pack1"], 0.45, (), 2)
    sq = [plan.copy(("sq", k), "d2d" if k == 4 else "q", 1024, 1) for k in range(1, NTP)]
    plan.task("spread", ["norm", *whole(IN[1:])], 0.6, sq, 1)
    plan.task("carrier", ["norm", *whole(IN[:1])], 0.5, (), 2)
    plan.task("mask", ["pack1"], 0.03, (), 3)
    plan.task("mixed", ["spread", "carrier", "mask", *[("sq", k) for k in range(1, NTP)]], 0.45, (), 1)

    half = 65536

    def scatter(w, deps, dur):
        last = deps
        for k in (2, 1, 3, 0):
            cp = plan.copy(("p", w, k), "d2d", 2 * half, 1)
            plan.task(("part", w, k), last, dur, (cp,), 1)
            last = [("part", w, k)]
        cps = [plan.copy(("c", w, 2, h), "x-" if h else "x+", half, 1) for h in (0, 1)]
        plan.task(("sum2", w), [("part", w, 2), ("p", w, 2)], dur + 0.1, cps, 1)
        for k, h in ((1, 1), (3, 0), (1, 0), (3, 1)):
            cp = plan.copy(("c", w, k, h), "x-" if k == 3 else "x+", half, 1)
            need = [("c", w, 2, h), ("sum", w, k, 1 - h)] if (k, h) in ((1, 0), (3, 1)) else [("sum2", w)]
            plan.task(("sum", w, k, h), [("part", w, k), *need, ("p", w, k)], dur * 0.6 + 0.1, (cp,), 1)
        plan.task(("own", w), [("part", w, 0), ("p", w, 0)], dur, (), 2)
        return [("own", w)] + [("c", w, k, h) for k in (1, 3) for h in (0, 1)]

    after = scatter(0, ["mixed", *whole(BLEND)], 0.2)
    ag = [plan.copy(("ac", k, h), "x-" if k == 3 else "x+", half, 1) for k, h in ((1, 0), (3, 1), (1, 1), (3, 0))]
    ag.append(plan.copy(("ap", 0, 0), "d2d", 2 * half, 1))
    plan.task("stream", after, 0.2, ag, 1)
    got = [("ap", 0, 0)]
    for k, h in ((1, 0), (3, 1), (1, 1), (3, 0), (2, 0), (2, 1)):
        cps = []
        if (k, h) in ((1, 0), (3, 1)):
            cps.append(plan.copy(("ac", 2, h), "x-" if h else "x+", half, 1))
        cps.append(plan.copy(("ap", k, h), "d2d", half, 1))
        plan.task(("pass", k, h), [("ac", k, h), "stream"], 0.03, cps, 0)
        got += [("pass", k, h), ("ap", k, h)]
    plan.task("norm2", ["stream", *got], 0.5, (), 1)
    plan.task("hidden", ["norm2", *whole(SE)], 1.3, (), 1)
    plan.task("unpack", [*whole(SE[-1:]), *whole(CON)], 0.5, (), 1)
    after = scatter(1, ["hidden", "unpack"], 0.3)
    plan.task("out", after, 0.3, (), 1)
    return plan


def kernel(
    plan,
    seq,
    *refs,
):
    hbm, out_ref, rest = refs[: len(NAMES)], refs[len(NAMES)], refs[len(NAMES) + 1 :]
    local, rest = rest[: len(NAMES)], rest[len(NAMES) :]
    (
        g,
        normed,
        carrier,
        spread,
        tail,
        sqbuf,
        opm,
        gated,
        active,
        psend,
        precv,
        csend,
        crecv,
        own,
        sbuf,
        scale,
        send_sem,
        recv_sem,
        load_sem,
    ) = rest
    (
        x_ref, gain1_ref, wprod_ref, sprod_ref, wplace_ref, splace_ref, gains_ref, op_ref, bias_ref,
        wblend_ref, sblend_ref, gain2_ref, wsw_ref, ssw_ref, wex_ref, sex_ref, wcon_ref, scon_ref,
    ) = local
    rep, fs, tp = lax.axis_index("rep"), lax.axis_index("fs"), lax.axis_index("tp")
    zl, y = fs // NY, lax.rem(fs, NY)
    x, core = tp // 2, lax.rem(tp, 2)
    z = rep * NZ + zl

    def at_z(d):
        zz = lax.rem(z + d + NREP * NZ, NREP * NZ)
        return {"rep": zz // NZ, "fs": lax.rem(zz, NZ) * NY + y}

    def at_y(d):
        return {"fs": zl * NY + lax.rem(y + d + NY, NY)}

    def at_tp(k):
        return {"tp": lax.rem(tp + k + NTP, NTP)}

    def at_x(k):
        return {"tp": lax.rem(x + k + NX, NX) * 2 + core}

    partner = {"tp": x * 2 + 1 - core}

    def slot(a):
        return lax.rem(zl - a[0] + NZ, NZ) * NY + lax.rem(y - a[1] + NY, NY)

    def send(key, src, dst, dev):
        pltpu.make_async_remote_copy(
            src_ref=src, dst_ref=dst, send_sem=send_sem.at[KINDS.index(key[0])], recv_sem=recv_sem.at[plan.copies[key]],
            device_id=dev, device_id_type=MESH,
        ).start()

    def arrive(key, dst, dev):
        pltpu.make_async_remote_copy(
            src_ref=dst, dst_ref=dst, send_sem=send_sem.at[KINDS.index(key[0])], recv_sem=recv_sem.at[plan.copies[key]],
            device_id=dev, device_id_type=MESH,
        ).wait_recv()

    arrs = [arrivals_of(s) for s in STREAMS]

    def block(s, a):
        return g.at[slot(a), pl.ds(STREAMS[s][0], STREAMS[s][1])]

    def forward(s, a):
        for b, (parent, axis, step) in arrs[s].items():
            if parent == a:
                send(("w", s, *b), block(s, a), block(s, a), at_z(step) if axis == "z" else at_y(step))

    zs = sorted({e * v[2] for a in arrs for v in a.values() if v[1] == "z" for e in (1, -1)})
    ys = sorted({(e * v[2]) % NY for a in arrs for v in a.values() if v[1] == "y" for e in (1, -1)})
    greet = [at_z(d) for d in zs] + [at_y(d) for d in ys] + [at_tp(k) for k in range(1, NTP)]
    barrier = pltpu.get_barrier_semaphore()
    for dev in greet:
        pl.semaphore_signal(barrier, inc=1, device_id=dev, device_id_type=MESH)

    def loading(name):
        i = NAMES.index(name)
        return pltpu.make_async_copy(hbm[i], local[i], load_sem.at[i])

    for name in LOADS:
        loading(name).start()

    def load(*names):
        for name in names:
            loading(name).wait()

    def pack1():
        load("wprod", "wplace")
        g[fs, R_PROD : R_PROD + 64, :] = wprod_ref[...].astype(BF16)
        g[fs, R_PLACE : R_PLACE + 64, :] = wplace_ref[...].astype(BF16)
        pl.semaphore_wait(barrier, len(greet))

    def packb():
        load("wblend", "sblend")
        wb = wblend_ref[...].astype(BF16).astype(F32) * jnp.broadcast_to(sblend_ref[...], (128, 64)).T
        g[fs, R_BLEND : R_BLEND + 64, :] = wb.astype(BF16)

    def pack2():
        load("wsw", "wex", "ssw", "sex")
        for i, w in ((0, wsw_ref), (2, wex_ref)):
            for j in (0, 1):
                g[fs, R_SE + 64 * (i + j) : R_SE + 64 * (i + j + 1), :] = w[:, 128 * j : 128 * (j + 1)].astype(BF16)
        load("wcon", "scon")
        by = jnp.broadcast_to(scon_ref[...], (128, 64)).T[:, 0:1]
        wc = (wcon_ref[...].astype(BF16).astype(F32) * by).astype(BF16)
        for i, w in ((0, wsw_ref), (1, wex_ref)):
            at = pl.ds(R_TAIL + 64 * i, 64)
            g[fs, at, 0:96] = w[:, 256:352].astype(BF16)
            g[fs, at, 96:128] = wc[:, 256 + 32 * i : 288 + 32 * i]
        g[fs, R_CON : R_CON + 64, :] = wc[:, 0:128]
        g[fs, R_CON + 64 : R_CON + 128, :] = wc[:, 128:256]
        for q in range(4):
            g[fs, R_CON + 128 : R_CON + 144, 32 * q : 32 * (q + 1)] = wc[16 * q : 16 * (q + 1), 320:352]
        scale[...] = jnp.zeros_like(scale)
        scale[0:1, 0:HID] = ssw_ref[...].reshape(1, HID)
        scale[1:2, 0:HID] = sex_ref[...].reshape(1, HID)

    def unpack():
        for i in (0, 1):
            tail[:, :, 32 * i : 32 * (i + 1)] = g[:, R_TAIL + 64 * i : R_TAIL + 64 * (i + 1), 96:128]
        for q in range(4):
            tail[:, 16 * q : 16 * (q + 1), 64:96] = g[:, R_CON + 128 : R_CON + 144, 32 * q : 32 * (q + 1)]

    def go(s):
        forward(s, (0, 0))

    def recv(s, dz, dy):
        _, axis, step = arrs[s][(dz, dy)]
        arrive(("w", s, dz, dy), block(s, (dz, dy)), at_z(-step) if axis == "z" else at_y(-step))
        forward(s, (dz, dy))

    def leaf(s):
        leaves = leaves_of(arrs[s])
        ref = g.at[0 : len(leaves), pl.ds(STREAMS[s][0], STREAMS[s][1])]
        arrive(("w", s, *leaves[0]), ref, at_y(1))

    def tile(row):
        return g[:, row : row + 64, :].reshape(DIM, 128)

    def norm():
        load("x", "gain1")
        v = x_ref[...].astype(F32)
        r = lax.rsqrt(jnp.mean(v * v, axis=-1, keepdims=True) + EPS)
        normed[...] = (v * r * gain1_ref[...]).astype(BF16)

    def spreading():
        load("splace")
        h = jnp.dot(normed[...], tile(R_PLACE), preferred_element_type=F32)
        sp = jax.nn.gelu(h * splace_ref[...])
        spread[...] = sp
        sqbuf[tp] = jnp.sum((sp * sp).T, axis=0, keepdims=True)
        for k in range(1, NTP):
            send(("sq", k), sqbuf.at[tp], sqbuf.at[tp], at_tp(k))

    def carry():
        load("sprod")
        h = jnp.dot(normed[...], tile(R_PROD), preferred_element_type=F32)
        carrier[...] = jax.nn.gelu(h * sprod_ref[...])

    def mask():
        load("op", "gains", "bias", "gain2")
        tail[...] = jnp.zeros_like(tail)
        t = lax.broadcasted_iota(jnp.int32, (BLOCK, BLOCK), 0)
        s = lax.broadcasted_iota(jnp.int32, (BLOCK, BLOCK), 1)
        opm[...] = jnp.where(t >= s, op_ref[tp].astype(F32), 0.0).astype(BF16)

    def mixed():
        for k in range(1, NTP):
            src = lax.rem(tp - k + NTP, NTP)
            arrive(("sq", k), sqbuf.at[src], at_tp(-k))
        total = jnp.sum(sqbuf[...], axis=0)
        r = lax.rsqrt(total / CH + EPS)
        r = jnp.broadcast_to(r, (128, TOK)).T
        sn = (spread[...] * r * gains_ref[...]).astype(BF16)
        bias = jnp.broadcast_to(bias_ref[pl.ds(tp, 1), :], (BLOCK, BLOCK)).T
        w = opm[...]
        for n in range(TOK // BLOCK):
            rows = slice(n * BLOCK, (n + 1) * BLOCK)
            m = jnp.dot(w, sn[rows], preferred_element_type=F32) + bias
            gated[rows, :] = (carrier[rows, :] * m).astype(BF16)

    nt = (((1,), (1,)), ((), ()))

    def product(w, d, r=slice(None)):
        if w == 0:
            b = g[pl.ds(4 * d, 4), R_BLEND : R_BLEND + 64, :].reshape(256, 128)
            return lax.dot_general(gated[r, :], b, nt, preferred_element_type=F32)
        cols = [g[pl.ds(4 * d, 4), R_CON + 64 * j : R_CON + 64 * (j + 1), :].reshape(256, 128) for j in (0, 1)]
        cols.append(tail[pl.ds(4 * d, 4)].reshape(256, 128))
        return lax.dot_general(active[r, :], jnp.concatenate(cols, axis=1), nt, preferred_element_type=F32)

    def chip(k):
        return lax.rem(x + k, NX) * 2

    def part(w, k):
        psend[w, k] = product(w, chip(k) + 1 - core).astype(BF16)
        send(("p", w, k), psend.at[w, k], precv.at[w, k], partner)

    def rows(h):
        return slice(128 * h, 128 * (h + 1))

    def sum2(w):
        v = product(w, chip(2) + core)
        arrive(("p", w, 2), precv.at[w, 2], partner)
        csend[w, 0] = (v + precv[w, 2].astype(F32)).astype(BF16)
        for h in (0, 1):
            send(("c", w, 2, h), csend.at[w, 0, rows(h)], crecv.at[w, 0, rows(h)], at_x(-1 if h else 1))

    def add(w, k, h):
        v = product(w, chip(k) + core, rows(h))
        if (k, h) in ((1, 1), (3, 0)):
            arrive(("p", w, k), precv.at[w, k], partner)
        v = v + precv[w, k, rows(h)].astype(F32)
        if (k, h) in ((1, 0), (3, 1)):
            arrive(("c", w, 2, h), crecv.at[w, 0, rows(h)], at_x(1 if h else -1))
            v = v + crecv[w, 0, rows(h)].astype(F32)
        i = 1 if k == 1 else 2
        csend[w, i, rows(h)] = v.astype(BF16)
        send(("c", w, k, h), csend.at[w, i, rows(h)], crecv.at[w, i, rows(h)], at_x(k))

    def keep(w):
        v = product(w, chip(0) + core)
        arrive(("p", w, 0), precv.at[w, 0], partner)
        own[...] = v + precv[w, 0].astype(F32)

    def total(w):
        v = own[...]
        for k in (1, 3):
            i = 1 if k == 1 else 2
            for h in (0, 1):
                arrive(("c", w, k, h), crecv.at[w, i, rows(h)], at_x(-k))
            v = v + crecv[w, i].astype(F32)
        return v

    def stream():
        mine = x_ref[:, pl.ds(pl.multiple_of(tp * 256, 256), 256)].astype(F32)
        sbuf[tp] = (mine + total(0)).astype(BF16)
        for k, h in ((1, 0), (3, 1), (1, 1), (3, 0)):
            send(("ac", k, h), sbuf.at[tp, rows(h)], sbuf.at[tp, rows(h)], at_x(k))
        send(("ap", 0, 0), sbuf.at[tp], sbuf.at[tp], partner)

    def relay(k, h):
        d = lax.rem(x - k + NX, NX) * 2 + core
        ref = sbuf.at[d, rows(h)]
        arrive(("ac", k, h), ref, at_x(-k) if k != 2 else at_x(1 if h else -1))
        if (k, h) in ((1, 0), (3, 1)):
            send(("ac", 2, h), ref, ref, at_x(-1 if h else 1))
        send(("ap", k, h), ref, ref, partner)

    def norm2():
        for k in range(4):
            d = lax.rem(x - k + NX, NX) * 2 + 1 - core
            if k == 0:
                arrive(("ap", 0, 0), sbuf.at[d], partner)
            else:
                for h in (0, 1):
                    arrive(("ap", k, h), sbuf.at[d, rows(h)], partner)
        sq = jnp.zeros((TOK, 256), F32)
        for d in range(NTP):
            v = sbuf[d].astype(F32)
            sq = sq + v * v
        r = lax.rsqrt(jnp.sum(sq, axis=-1, keepdims=True) / DIM + EPS)
        for d in range(NTP):
            cols = slice(256 * d, 256 * (d + 1))
            normed[:, cols] = (sbuf[d].astype(F32) * r * gain2_ref[:, cols]).astype(BF16)

    def hidden():
        for j, (a, b) in enumerate(((0, 2), (1, 3), (4, 5))):
            w = jnp.concatenate([tile(R_SE + 64 * a), tile(R_SE + 64 * b)], axis=1)
            h = jnp.dot(normed[...], w, preferred_element_type=F32)
            cols = slice(128 * j, 128 * (j + 1))
            gate = h[:, 0:128] * scale[0:1, cols]
            up = h[:, 128:256] * scale[1:2, cols]
            active[:, cols] = (gate / (1.0 + jnp.exp(-gate)) * up).astype(BF16)

    def out():
        out_ref[...] = (sbuf[tp].astype(F32) + total(1)).astype(BF16)

    run = {
        "pack1": pack1, "packb": packb, "pack2": pack2, "go": go, "norm": norm, "spread": spreading, "carrier": carry, "unpack": unpack, "mask": mask, "mixed": mixed, "stream": stream,
        "norm2": norm2, "hidden": hidden, "out": out, "recv": recv, "leaf": leaf, "part": part, "sum": add, "sum2": sum2, "own": keep, "pass": relay,
    }
    for key, _ in seq:
        if isinstance(key, tuple):
            run[key[0]](*key[1:])
        else:
            run[key]()
    for i, all_sent in enumerate((g.at[0:31], sqbuf.at[0:7], psend, csend, sbuf.at[0:3], sbuf.at[0:4])):
        pltpu.make_async_copy(all_sent, all_sent, send_sem.at[i]).wait()


def on_device(*args):
    plan = make_plan()
    seq = plan.order()
    n = len(plan.groups)
    args = list(args)
    for i in (NAMES.index("wblend"), NAMES.index("wcon")):
        args[i] = args[i].T
    args = [a.reshape(1, -1) if a.ndim == 1 and a.size != HID else a for a in args]
    return pl.pallas_call(
        functools.partial(kernel, plan, seq),
        out_shape=jax.ShapeDtypeStruct((TOK, 256), BF16),
        in_specs=[pl.BlockSpec(memory_space=pltpu.HBM)] * len(args),
        out_specs=pl.BlockSpec(memory_space=pltpu.VMEM),
        scratch_shapes=[
            *[pltpu.VMEM(a.shape, a.dtype) for a in args],
            pltpu.VMEM((NY * NZ, R_ALL, 128), BF16),
            pltpu.VMEM((TOK, DIM), BF16),
            pltpu.VMEM((TOK, 128), F32),
            pltpu.VMEM((TOK, 128), F32),
            pltpu.VMEM((NY * NZ, 64, 128), BF16),
            pltpu.VMEM((NTP, 1, TOK), F32),
            pltpu.VMEM((BLOCK, BLOCK), BF16),
            pltpu.VMEM((TOK, 128), BF16),
            pltpu.VMEM((TOK, 384), BF16),
            pltpu.VMEM((2, 4, TOK, 256), BF16),
            pltpu.VMEM((2, 4, TOK, 256), BF16),
            pltpu.VMEM((2, 3, TOK, 256), BF16),
            pltpu.VMEM((2, 3, TOK, 256), BF16),
            pltpu.VMEM((TOK, 256), F32),
            pltpu.VMEM((NTP, TOK, 256), BF16),
            pltpu.VMEM((8, 384), F32),
            pltpu.SemaphoreType.DMA((len(KINDS),)),
            pltpu.SemaphoreType.DMA((n,)),
            pltpu.SemaphoreType.DMA((len(args),)),
        ],
        compiler_params=pltpu.CompilerParams(
            collective_id=0, has_side_effects=True, vmem_limit_bytes=67043328
        ),
        name="layer",
    )(*args)


def solution(mesh):
    return jax.shard_map(
        on_device,
        mesh=mesh,
        in_specs=(
            P(("rep", "fs"), None),
            P(),
            P("fs", "tp"),
            P("tp"),
            P("fs", "tp"),
            P("tp"),
            P("tp"),
            P(),
            P(),
            P("tp", "fs"),
            P("fs"),
            P(),
            P("fs", "tp"),
            P("tp"),
            P("fs", "tp"),
            P("tp"),
            P("tp", "fs"),
            P("fs"),
        ),
        out_specs=P(("rep", "fs"), "tp"),
        check_vma=False,
    )
```
